256 devices in a mesh: ep: 64 (over z, y, core), tp: 4 (over x).
Axes of the slice: x: 4, y: 4, z: 8, core: 2. Of those that a mesh axis runs over, the one named last changes fastest.
Arguments:
- mixer_in: bfloat16 [32768, 4096], P(('ep', 'tp')), may hold values from -6 to 6
- mixer_gain: float32 [4096], replicated, may hold values from 0.1 to 1.9
- group_weight: bfloat16 [4, 1024, 1024], P('tp'), may hold values from -0.1875 to 0.1875
- group_scale: float32 [4, 1024], P('tp'), may hold values from 0.1 to 1.9
- expert_in: bfloat16 [32768, 4096], P(('ep', 'tp')), may hold values from -6 to 6
- expert_gain: float32 [4096], replicated, may hold values from 0.1 to 1.9
- routes: int32 [32768, 2], P('ep'), may hold values from 0 to 63, all different within a row; in each aligned block of 128 rows (0 to 127, 128 to 255, ...) at most 6 rows name the same one
- route_weight: float32 [32768, 2], P('ep'), may hold values from 0.2 to 1
- gate_weight: bfloat16 [64, 4096, 1024], P('ep', None, 'tp'), may hold values from -0.25 to 0.25
- up_weight: bfloat16 [64, 4096, 1024], P('ep', None, 'tp'), may hold values from -0.25 to 0.25
- down_weight: bfloat16 [64, 1024, 4096], P('ep', 'tp'), may hold values from -0.02734375 to 0.02734375
Outputs:
- mixed: bfloat16 [32768, 4096], P('ep', 'tp')
- expert_out: bfloat16 [32768, 4096], P(('ep', 'tp'))
The draws below stay inside these ranges and needn't reach their ends.
Inputs may be any that keep to these rules, and one draw needn't show every extreme that they name: `routes`: each row names 2 different experts; within the rows of one device (aligned blocks of 128 rows) no expert is named more than 6 times, and that count is reached.
All inputs are finite; a program needn't handle non-finite values.
Results may differ from the reference program's by a relative error of at most 0.012.
Values may be sent and summed in bfloat16 or wider, within the bound.
A program may use at most 128 MiB of HBM per device.

```python
import math
import jax
import jax.numpy as jnp
import numpy as np
from jax import lax

D = 4096
GROUPS = 4
GW = 1024
WMAX = 16
F = 1024
TOP = 2
TOK_B = 128
EXPERTS = 64
CAP = 6
TOKENS_A = 32768
TOKENS_B = 32768
N_TP = 4


def levels(rng, dims, cuts, low, high):
    loudness, own = 1.0, jax.random.fold_in(rng, 6)
    for axis_at, blocks in cuts:
        steps = jnp.exp(jax.random.uniform(jax.random.fold_in(own, axis_at), (blocks,), jnp.float32, low / len(cuts), high / len(cuts)))
        loudness = loudness * jnp.repeat(steps, dims[axis_at] // blocks).reshape([-1 if axis == axis_at else 1 for axis in range(len(dims))])
    return loudness


def assign_block(rng, own, number, rows, amount, top, bound, slope):
    ranking = jax.random.permutation(rng, amount)
    packed, ordinary = portions_of(amount, rows * top, bound, slope, True), portions_of(amount, rows * top, bound, slope, False)
    places = jnp.arange(amount)

    def named(tallies, offset_by):
        used = int((tallies > 0).sum())
        fixed = max(1, used // 4)
        shifted = fixed + (places - fixed + offset_by * (used - fixed)) % max(1, amount - fixed)
        return jnp.zeros((amount,), jnp.int32).at[ranking[jnp.where(places < fixed, places, shifted)]].set(jnp.asarray(tallies, jnp.int32))

    tallies = jnp.where(number % 4 == 0, named(packed, number // 4), named(ordinary, number - number // 4 - 1))
    mixed = jax.random.permutation(jax.random.fold_in(own, 3), amount)
    source_of, receiver = mixed[0:amount // 2 * 2:2], mixed[1:amount // 2 * 2:2]
    slack = jnp.minimum(tallies[source_of] - 1, bound - tallies[receiver]) // 2
    slack = jnp.where((source_of == ranking[0]) | (receiver == ranking[0]) | (tallies[receiver] == 0), 0, jnp.maximum(slack, 0))
    shifted = jax.random.randint(jax.random.fold_in(own, 4), (amount // 2,), 0, 1 << 20) % (slack + 1)
    tallies = tallies.at[source_of].add(-shifted).at[receiver].add(shifted)
    members = jnp.searchsorted(jnp.cumsum(tallies), jnp.arange(rows * top), side="right").astype(jnp.int32)
    listing = members.reshape(top, rows).T
    listing = listing[jax.random.permutation(jax.random.fold_in(own, 1), rows)]
    offset_by = jax.random.randint(jax.random.fold_in(own, 2), (rows, 1), 0, top)
    return jnp.take_along_axis(listing, (jnp.arange(top)[None, :] + offset_by) % top, axis=1)


def portions_of(amount, total, bound, skew, full):
    portions = [(1 << 20) // math.isqrt(rank ** skew) + 1 for rank in range(1, amount + 1)]
    largest = bound if full else min(bound, max(-(-total // amount), total * portions[0] // sum(portions)))
    least = 1 if total - largest >= amount - 1 else 0
    given, surplus = [largest] + [least] * (amount - 1), total - largest - least * (amount - 1)
    while surplus > 0:
        movable = [i for i in range(1, amount) if given[i] < largest] or [i for i in range(1, amount) if given[i] < bound]
        mass, budget = sum([portions[i] for i in movable]), surplus
        for i in movable:
            more = min(bound - given[i], max(1, budget * portions[i] // mass), surplus)
            given[i] = given[i] + more
            surplus = surplus - more
    return np.array(given)


def bell_draw(own_key, extent, width, bound, cuts=(), kind=jnp.bfloat16):
    result = width * jax.random.normal(own_key, extent, jnp.float32)
    if cuts:
        result = result * levels(own_key, extent, cuts, -0.22, 0.18)
    return jnp.clip(result, -bound, bound).astype(kind)


def setup_inputs(seed: int = 0) -> dict:
    key_of = jax.random.split(jax.random.key(seed), 12)
    mixer_in = bell_draw(key_of[0], (TOKENS_A, D), 1.0, 6.0, ((0, 256),))
    mixer_gain = jnp.clip(1.0 + 0.18 * jax.random.normal(key_of[1], (D,), jnp.float32), 0.1, 1.9)
    group_weight = bell_draw(key_of[2], (GROUPS, GW, GW), GW ** -0.5, 0.1875, ((0, 4),))
    group_scale = jnp.clip(1.0 + 0.18 * jax.random.normal(key_of[3], (GROUPS, GW), jnp.float32), 0.1, 1.9)
    expert_in = bell_draw(key_of[4], (TOKENS_B, D), 1.0, 6.0, ((0, 256),))
    expert_gain = jnp.clip(1.0 + 0.18 * jax.random.normal(key_of[5], (D,), jnp.float32), 0.1, 1.9)
    routes_keys = jax.random.split(jax.random.fold_in(key_of[6], 1), TOKENS_B // TOK_B)
    routes_turns = jax.random.permutation(jax.random.fold_in(key_of[6], 3), TOKENS_B // TOK_B)
    routes = jax.vmap(lambda own, number: assign_block(jax.random.fold_in(key_of[6], 2), own, number, TOK_B, EXPERTS, TOP, CAP, 2))(routes_keys, routes_turns).reshape((TOKENS_B, TOP))
    route_weight = jnp.clip(0.2 + 0.8 * jax.random.uniform(key_of[7], (TOKENS_B, TOP), jnp.float32) ** levels(key_of[7], (TOKENS_B, TOP), ((0, 64),), -0.2, 0.2), 0.2, 1.0)
    gate_weight = bell_draw(key_of[8], (EXPERTS, D, F), (D // 9) ** -0.5, 0.25, ((0, 64), (2, 4)))
    up_weight = bell_draw(key_of[9], (EXPERTS, D, F), (D // 9) ** -0.5, 0.25, ((0, 64), (2, 4)))
    down_weight = bell_draw(key_of[10], (EXPERTS, F, D), (45 * F) ** -0.5, 0.02734375, ((0, 64), (1, 4)))
    return {"mixer_in": mixer_in, "mixer_gain": mixer_gain, "group_weight": group_weight, "group_scale": group_scale, "expert_in": expert_in, "expert_gain": expert_gain, "routes": routes, "route_weight": route_weight, "gate_weight": gate_weight, "up_weight": up_weight, "down_weight": down_weight}


epsilon = 1e-06
clamp_limit = 7.0
sigmoid_slope = 1.702

def rms_norm(values, gain):
    widened = values.astype(jnp.float32)
    scaled = widened * lax.rsqrt(lax.optimization_barrier(jnp.mean(widened * widened, axis=-1, keepdims=True)) + epsilon)
    return (scaled * gain).astype(jnp.bfloat16)

def clamped_unit(gate_part, up_part):
    gate_part = jnp.minimum(gate_part, clamp_limit)
    up_part = jnp.clip(up_part, -clamp_limit, clamp_limit)
    return ((up_part + 1.0) * gate_part * jax.nn.sigmoid(sigmoid_slope * gate_part)).astype(jnp.bfloat16)

def slot_table(block_routes, experts, capacity):
    count = block_routes.shape[0]
    onehot = (block_routes[:, :, None] == jnp.arange(experts, dtype=jnp.int32)[None, None, :]).astype(jnp.int32)
    per_token = lax.optimization_barrier(jnp.sum(onehot, axis=1))
    earlier = jnp.cumsum(per_token, axis=0) - per_token
    slot_rank = lax.optimization_barrier(jnp.sum(onehot * earlier[:, None, :], axis=2))
    matches = onehot[:, :, :, None] * (slot_rank[:, :, None, None] == jnp.arange(capacity, dtype=jnp.int32)[None, None, None, :]).astype(jnp.int32)
    source = lax.optimization_barrier(jnp.sum(matches * jnp.arange(count, dtype=jnp.int32)[:, None, None, None], axis=(0, 1)))
    filled = lax.optimization_barrier(jnp.sum(matches, axis=(0, 1)))
    return (source, filled, slot_rank)

def reference(mixer_in, mixer_gain, group_weight, group_scale, expert_in, expert_gain, routes, route_weight, gate_weight, up_weight, down_weight):
    normed = rms_norm(mixer_in, mixer_gain)
    length = normed.shape[0]
    position = jnp.arange(length, dtype=jnp.int32)
    pieces = []
    for group in range(GROUPS):
        window = 2 ** (group + 1)
        values = normed[:, group * GW:(group + 1) * GW].astype(jnp.float32)
        padded = jnp.pad(values, ((WMAX - 1, 0), (0, 0)))
        window_sum = jnp.zeros_like(values)
        for offset in range(window):
            window_sum = window_sum + padded[WMAX - 1 - offset:WMAX - 1 - offset + length]
        counts = jnp.minimum(position + 1, window).astype(jnp.float32)[:, None]
        pooled = (window_sum / counts - values).astype(jnp.bfloat16)
        product = jnp.dot(pooled, group_weight[group], preferred_element_type=jnp.float32)
        pieces.append((product * group_scale[group]).astype(jnp.bfloat16))
    mixed = jnp.concatenate(pieces, axis=1)
    expert_norm = rms_norm(expert_in, expert_gain)
    blocks = expert_norm.shape[0] // TOK_B
    block_routes = routes.reshape(blocks, TOK_B, TOP)
    source, filled, slot_rank = lax.map(lambda item: slot_table(item, EXPERTS, CAP), block_routes)
    global_index = source + (jnp.arange(blocks, dtype=jnp.int32) * TOK_B)[:, None, None]
    part_width = F // N_TP

    def one_expert(expert):
        slot_index = lax.dynamic_index_in_dim(global_index, expert, 1, keepdims=False).reshape(-1)
        present = lax.dynamic_index_in_dim(filled, expert, 1, keepdims=False).reshape(-1)
        picked = expert_norm[slot_index] * present[:, None].astype(jnp.bfloat16)
        gate_part = jnp.dot(picked, gate_weight[expert], preferred_element_type=jnp.float32)
        up_part = jnp.dot(picked, up_weight[expert], preferred_element_type=jnp.float32)
        hidden = clamped_unit(gate_part, up_part)
        total = jnp.zeros((picked.shape[0], picked.shape[1]), jnp.float32)
        for part in range(N_TP):
            partial_value = jnp.dot(hidden[:, part * part_width:(part + 1) * part_width], down_weight[expert][part * part_width:(part + 1) * part_width], preferred_element_type=jnp.float32).astype(jnp.bfloat16)
            total = total + lax.optimization_barrier(partial_value).astype(jnp.float32)
        return total.astype(jnp.bfloat16).reshape(blocks, CAP, picked.shape[1])
    results = lax.map(one_expert, jnp.arange(EXPERTS, dtype=jnp.int32))
    flat_rows = results.reshape(-1, results.shape[-1])
    block_of = (jnp.arange(expert_norm.shape[0], dtype=jnp.int32) // TOK_B)[:, None]
    slot_index = (routes * blocks + block_of) * CAP + slot_rank.reshape(-1, TOP)
    expert_sum = jnp.zeros(expert_norm.shape, jnp.float32)
    for choice_slot in range(TOP):
        expert_sum = expert_sum + flat_rows[slot_index[:, choice_slot]].astype(jnp.float32) * route_weight[:, choice_slot:choice_slot + 1]
    return (mixed, expert_sum.astype(jnp.bfloat16))
```

```python
import functools

import jax
import jax.numpy as jnp
from jax import lax
from jax.experimental import pallas as pl
from jax.experimental.pallas import tpu as pltpu
from jax.sharding import PartitionSpec as P

WMAX = 16
TOP = 2
HALO = 128
epsilon = 1e-06
clamp_limit = 7.0
sigmoid_slope = 1.702
MESH = pl.DeviceIdType.MESH
f32 = jnp.float32
bf16 = jnp.bfloat16


def aligned(value, by):
    return pl.multiple_of(value, by)


def dot(a, b):
    return jnp.dot(a, b, preferred_element_type=f32)


def layer_kernel(
    dims,
    ein, egain, min_, mgain, routes, weights, scale, perm,
    gw_hbm, g_hbm, u_hbm, d_hbm,
    mixed_hbm, out_hbm,
    en, zsend, zrecv, ysend, xs, wg, wu, wd, acc, hid,
    psend, precv, rsend, rmid, rperm, rfin, pick, mix_hi, mix_lo,
    msend, ext, gw, mixed_buf, out_buf,
    lsem, osem, ssem, zr, yr, tr, wgr, wur, wdr, pr, rr, fr, mr,
):
    NZ, NJ, TOK, D, C, CAP, FL = dims
    NC = D // C
    E = NZ * NJ
    S = E * CAP
    BJ, BZ = NJ * CAP, NZ * CAP
    GW = D // 4
    ep = lax.axis_index("ep")
    t = lax.axis_index("tp")
    z = ep // NJ
    j = ep % NJ
    t_mate = t + 1 - 2 * (t % 2)
    w_mate = 3 - t

    def remote(src, dst, send, recv, e, tt):
        return pltpu.make_async_remote_copy(
            src_ref=src, dst_ref=dst, send_sem=send, recv_sem=recv,
            device_id=(e, tt), device_id_type=MESH,
        )

    def drain(src, dst, sem):
        pltpu.make_async_copy(src, dst, sem).wait()

    barrier = pltpu.get_barrier_semaphore()

    def hello(e, tt):
        pl.semaphore_signal(barrier, inc=1, device_id=(e, tt), device_id_type=MESH)

    lax.fori_loop(1, NZ, lambda k, _: (hello(((z + k) % NZ) * NJ + j, t), 0)[1], 0)
    lax.fori_loop(1, NJ, lambda k, _: (hello(z * NJ + (j + k) % NJ, t), 0)[1], 0)
    lax.fori_loop(1, 4, lambda k, _: (hello(ep, (t + k) % 4), 0)[1], 0)

    @pl.when(ep > 0)
    def _():
        hello(ep - 1, 3)

    own_g = pltpu.make_async_copy(g_hbm.at[0], wg.at[0], lsem.at[0])
    own_u = pltpu.make_async_copy(u_hbm.at[0], wu.at[0], lsem.at[1])
    own_w = pltpu.make_async_copy(gw_hbm.at[0], gw, lsem.at[3])
    own_g.start()
    own_u.start()
    own_w.start()

    def own_d(c):
        return pltpu.make_async_copy(
            d_hbm.at[0, :, pl.ds(aligned(c * C, C), C)], wd.at[c, pl.ds(0, FL)], lsem.at[2]
        )

    def start_own_d(c, _):
        own_d(c).start()
        return 0

    lax.fori_loop(0, NC, start_own_d, 0)

    def norm_rows(src, gain, i):
        rows = pl.ds(aligned(i * 16, 16), 16)
        values = src[rows, :].astype(f32)
        mean = jnp.mean(values * values, axis=-1, keepdims=True)
        return rows, (values * lax.rsqrt(mean + epsilon) * gain[...]).astype(bf16)

    def expert_rows(i, _):
        rows, values = norm_rows(ein, egain, i)
        for c in range(NC):
            en[c, rows, :] = values[:, c * C : (c + 1) * C]
        return 0

    lax.fori_loop(0, TOK // 16, expert_rows, 0)

    own = pl.ds(aligned(t * TOK, TOK), TOK)
    r0, r1 = routes[0:1, own], routes[1:2, own]
    w0, w1 = weights[0:1, own], weights[1:2, own]
    experts = lax.broadcasted_iota(jnp.int32, (E, TOK), 0)
    is0, is1 = experts == r0, experts == r1
    named = jnp.where(is0 | is1, 1.0, 0.0).astype(bf16)
    tri = jnp.where(
        lax.broadcasted_iota(jnp.int32, (TOK, TOK), 0)
        < lax.broadcasted_iota(jnp.int32, (TOK, TOK), 1),
        1.0,
        0.0,
    ).astype(bf16)
    earlier = dot(named, tri)
    rank0 = jnp.sum(jnp.where(is0, earlier, 0.0), axis=0, keepdims=True)
    rank1 = jnp.sum(jnp.where(is1, earlier, 0.0), axis=0, keepdims=True)
    slot0 = r0 * CAP + rank0.astype(jnp.int32)
    slot1 = r1 * CAP + rank1.astype(jnp.int32)
    slots = lax.broadcasted_iota(jnp.int32, (S, TOK), 0)
    at0, at1 = slots == slot0, slots == slot1
    pick[...] = jnp.where(at0 | at1, 1.0, 0.0).astype(bf16)
    share = (jnp.where(at0, w0, 0.0) + jnp.where(at1, w1, 0.0)).T
    high = share.astype(bf16)
    mix_hi[...] = high
    mix_lo[...] = (share - high.astype(f32)).astype(bf16)

    last = ((t + 1) // 4) * (1 - (ep + 1) // E)
    pl.semaphore_wait(barrier, (NZ - 1) + (NJ - 1) + 3 + 4 * last)

    def z_copy(c, k):
        there = (z + k) % NZ
        return remote(
            zsend.at[c, there], zrecv.at[c, z], ssem.at[0], zr.at[c], there * NJ + j, t
        )

    def start_z(c, _):
        zsend[c] = dot(pick[...], en[c]).astype(bf16).reshape(NZ, BJ, C)
        zrecv[c, z] = zsend[c, z]
        lax.fori_loop(1, NZ, lambda k, _: (z_copy(c, k).start(), 0)[1], 0)
        return 0

    def wg_copy(c):
        rows = pl.ds(aligned(c * C, C), C)
        return remote(g_hbm.at[0, rows], wg.at[1, rows], ssem.at[1], wgr.at[c], ep, w_mate)

    def wu_copy(c):
        rows = pl.ds(aligned(c * C, C), C)
        return remote(u_hbm.at[0, rows], wu.at[1, rows], ssem.at[2], wur.at[c], ep, w_mate)

    def wd_copy(c):
        return remote(
            d_hbm.at[0, :, pl.ds(aligned(c * C, C), C)], wd.at[c, pl.ds(FL, FL)],
            ssem.at[3], wdr.at[c], ep, w_mate,
        )

    def start_w(c, _):
        wg_copy(c).start()
        wu_copy(c).start()
        return 0

    start_z(0, 0)
    lax.fori_loop(0, NC, start_w, 0)
    lax.fori_loop(0, NC, lambda c, _: (wd_copy(c).start(), 0)[1], 0)
    lax.fori_loop(1, NC, start_z, 0)

    def mixer_rows(i, _):
        rows, values = norm_rows(min_, mgain, i)
        for g in range(4):
            msend[g, rows, :] = values[:, g * GW : (g + 1) * GW]
        return 0

    lax.fori_loop(0, TOK // 16, mixer_rows, 0)

    def m_copy(k):
        there = (t + k) % 4
        return remote(
            msend.at[there], ext.at[pl.ds(aligned(HALO + t * TOK, 16), TOK)],
            ssem.at[4], mr.at[0], ep, there,
        )

    def halo_copy(g):
        return remote(
            msend.at[g, pl.ds(TOK - WMAX, WMAX)], ext.at[pl.ds(HALO - WMAX, WMAX)],
            ssem.at[5], mr.at[1], ep + 1, g,
        )

    lax.fori_loop(1, 4, lambda k, _: (m_copy(k).start(), 0)[1], 0)
    ext[0 : HALO - WMAX] = jnp.zeros((HALO - WMAX, GW), bf16)
    ext[pl.ds(aligned(HALO + t * TOK, 16), TOK), :] = msend[t]

    @pl.when((t == 3) & (ep < E - 1))
    def _():
        lax.fori_loop(0, 4, lambda g, _: (halo_copy(g).start(), 0)[1], 0)

    @pl.when(ep == 0)
    def _():
        ext[HALO - WMAX : HALO] = jnp.zeros((WMAX, GW), bf16)

    def clear(k, _):
        acc[k // 4, k % 4] = jnp.zeros((S, FL), f32)
        return 0

    lax.fori_loop(0, 8, clear, 0)

    def y_copy(c, k):
        there = (j + k) % NJ
        return remote(
            ysend.at[c, there], xs.at[0, c, j], ssem.at[6], yr.at[c], z * NJ + there, t
        )

    def stage_y(c):
        drain(zsend.at[c, pl.ds(0, NZ - 1)], zrecv.at[c, pl.ds(0, NZ - 1)], zr.at[c])
        moved = dot(perm[...], zrecv[c].reshape(S, C)).astype(bf16)
        ysend[c] = moved.reshape(NJ, BZ, C)
        xs[0, c, j] = ysend[c, j]
        lax.fori_loop(1, NJ, lambda k, _: (y_copy(c, k).start(), 0)[1], 0)

    def t_copy(c):
        return remote(xs.at[0, c], xs.at[1, c], ssem.at[7], tr.at[c], ep, t_mate)

    def stage_t(c):
        drain(ysend.at[c, pl.ds(0, NJ - 1)], xs.at[0, c, pl.ds(0, NJ - 1)], yr.at[c])
        t_copy(c).start()

    def stage_in(c):
        t_copy(c).wait_recv()
        wg_copy(c).wait_recv()
        wu_copy(c).wait_recv()
        rows = pl.ds(aligned(c * C, C), C)

        def half(h, _):
            x = xs[h, c].reshape(S, C)
            for part in range(2):
                acc[h, part] += dot(x, wg[part, rows, :])
                acc[h, 2 + part] += dot(x, wu[part, rows, :])
            return 0

        lax.fori_loop(0, 2, half, 0)

    def mixer():
        own_w.wait()

        def wait_peer(k, _):
            m_copy(k).wait_recv()
            return 0

        drain(msend.at[pl.ds(0, 3)], msend.at[pl.ds(0, 3)], mr.at[0])

        @pl.when(ep > 0)
        def _():
            drain(
                msend.at[0, pl.ds(0, WMAX)], ext.at[pl.ds(HALO - WMAX, WMAX)], mr.at[1]
            )

        window = jnp.left_shift(2, t)
        row = lax.broadcasted_iota(jnp.int32, (TOK, HALO + TOK), 0) + HALO
        col = lax.broadcasted_iota(jnp.int32, (TOK, HALO + TOK), 1)
        band = jnp.where((col <= row) & (col > row - window), 1.0, 0.0).astype(bf16)

        def block(b, _):
            start = aligned(b * TOK, TOK)
            sums = dot(band, ext[pl.ds(start, HALO + TOK), :])
            place = ep * (4 * TOK) + start + lax.broadcasted_iota(jnp.int32, (TOK, 1), 0)
            count = jnp.minimum(place + 1, window).astype(f32)
            center = ext[pl.ds(aligned(start + HALO, TOK), TOK), :].astype(f32)
            pooled = (sums / count - center).astype(bf16)
            mixed_buf[pl.ds(start, TOK), :] = (dot(pooled, gw[...]) * scale[...]).astype(bf16)
            return 0

        lax.fori_loop(0, 4, block, 0)
        pltpu.make_async_copy(mixed_buf, mixed_hbm, osem.at[0]).start()

    LAG = 3

    def step_in(i, _):
        @pl.when(i < NC)
        def _():
            stage_y(i)

        @pl.when(i == LAG)
        def _():
            own_g.wait()
            own_u.wait()

        @pl.when(i >= LAG)
        def _():
            stage_in(i - LAG)

        @pl.when(i < NC)
        def _():
            stage_t(i)

        @pl.when(i == 1)
        def _():
            mixer()

        return 0

    lax.fori_loop(0, NC + LAG, step_in, 0)

    def units(b, _):
        rows = pl.ds(aligned(b * 64, 64), 64)
        for h in range(2):
            for part in range(2):
                gate = jnp.minimum(acc[h, part, rows, :], clamp_limit)
                up = jnp.clip(acc[h, 2 + part, rows, :], -clamp_limit, clamp_limit)
                hid[h, rows, part * FL : (part + 1) * FL] = (
                    (up + 1.0) * gate * jax.nn.sigmoid(sigmoid_slope * gate)
                ).astype(bf16)
        return 0

    lax.fori_loop(0, S // 64, units, 0)

    def p_copy(c):
        return remote(psend.at[c], precv.at[c], ssem.at[8], pr.at[c], ep, t_mate)

    def stage_part(c):
        wd_copy(c).wait_recv()
        psend[c] = dot(hid[1], wd[c]).astype(bf16)
        p_copy(c).start()

    def r_copy(c, k):
        there = (j + k) % NJ
        return remote(
            rsend.at[c, there], rmid.at[c, j], ssem.at[9], rr.at[c], z * NJ + there, t
        )

    def stage_result(c):
        mine = dot(hid[0], wd[c])
        p_copy(c).wait_recv()
        rsend[c] = (mine + precv[c].astype(f32)).astype(bf16).reshape(NJ, BZ, C)
        rmid[c, j] = rsend[c, j]
        lax.fori_loop(1, NJ, lambda k, _: (r_copy(c, k).start(), 0)[1], 0)

    def f_copy(c, k):
        there = (z + k) % NZ
        return remote(
            rperm.at[c, there], rfin.at[c, z], ssem.at[10], fr.at[c], there * NJ + j, t
        )

    def stage_back(c):
        drain(rsend.at[c, pl.ds(0, NJ - 1)], rmid.at[c, pl.ds(0, NJ - 1)], rr.at[c])
        moved = dot(perm[...], rmid[c].reshape(S, C)).astype(bf16)
        rperm[c] = moved.reshape(NZ, BJ, C)
        rfin[c, z] = rperm[c, z]
        lax.fori_loop(1, NZ, lambda k, _: (f_copy(c, k).start(), 0)[1], 0)

    def out_copy(c):
        return pltpu.make_async_copy(
            out_buf.at[c], out_hbm.at[:, pl.ds(aligned(c * C, C), C)], osem.at[1]
        )

    def stage_out(c):
        drain(rperm.at[c, pl.ds(0, NZ - 1)], rfin.at[c, pl.ds(0, NZ - 1)], fr.at[c])
        rows = rfin[c].reshape(S, C)
        out_buf[c] = (dot(mix_hi[...], rows) + dot(mix_lo[...], rows)).astype(bf16)
        out_copy(c).start()

    lax.fori_loop(0, NC, lambda c, _: (own_d(c).wait(), 0)[1], 0)

    def step_out(i, _):
        @pl.when(i < NC)
        def _():
            stage_part(i)

        @pl.when((i >= 2) & (i < NC + 2))
        def _():
            stage_result(i - 2)

        @pl.when((i >= 3) & (i < NC + 3))
        def _():
            stage_back(i - 3)

        @pl.when(i >= 5)
        def _():
            stage_out(i - 5)

        return 0

    lax.fori_loop(0, NC + 5, step_out, 0)

    drain(zsend.at[:, pl.ds(0, NZ - 1)], zrecv.at[:, pl.ds(0, NZ - 1)], ssem.at[0])
    drain(wg.at[1], wg.at[1], ssem.at[1])
    drain(wu.at[1], wu.at[1], ssem.at[2])
    drain(wd.at[:, pl.ds(FL, FL)], wd.at[:, pl.ds(FL, FL)], ssem.at[3])
    drain(msend.at[pl.ds(0, 3)], msend.at[pl.ds(0, 3)], ssem.at[4])

    @pl.when((t == 3) & (ep < E - 1))
    def _():
        drain(msend.at[:, pl.ds(0, WMAX)], msend.at[:, pl.ds(0, WMAX)], ssem.at[5])

    drain(ysend.at[:, pl.ds(0, NJ - 1)], ysend.at[:, pl.ds(0, NJ - 1)], ssem.at[6])
    drain(xs.at[0], xs.at[1], ssem.at[7])
    drain(psend, precv, ssem.at[8])
    drain(rsend.at[:, pl.ds(0, NJ - 1)], rsend.at[:, pl.ds(0, NJ - 1)], ssem.at[9])
    drain(rperm.at[:, pl.ds(0, NZ - 1)], rperm.at[:, pl.ds(0, NZ - 1)], ssem.at[10])
    pltpu.make_async_copy(mixed_buf, mixed_hbm, osem.at[0]).wait()
    lax.fori_loop(0, NC, lambda c, _: (out_copy(c).wait(), 0)[1], 0)


def shards(
    mixer_in, mixer_gain, group_weight, group_scale, expert_in, expert_gain,
    routes, route_weight, gate_weight, up_weight, down_weight,
):
    E = lax.axis_size("ep")
    NJ = 8 if E == 64 else 2
    NZ = E // NJ
    TOK, D = expert_in.shape
    CAP = max(2, 3 * TOK * TOP // (2 * E))
    S = E * CAP
    FL = gate_weight.shape[2]
    NC = 8 if D >= 4096 else 4
    C = D // NC
    GW = D // 4
    BJ, BZ = NJ * CAP, NZ * CAP
    index = jnp.arange(S, dtype=jnp.int32)
    swapped = (index // CAP % NJ) * BZ + (index // BJ) * CAP + index % CAP
    perm = (swapped[:, None] == index[None, :]).astype(bf16)
    vmem = pl.BlockSpec(memory_space=pltpu.VMEM)
    hbm = pl.BlockSpec(memory_space=pl.ANY)
    dma = pltpu.SemaphoreType.DMA
    buf = lambda *shape: pltpu.VMEM(shape, bf16)
    return pl.pallas_call(
        functools.partial(layer_kernel, (NZ, NJ, TOK, D, C, CAP, FL)),
        out_shape=(
            jax.ShapeDtypeStruct((4 * TOK, GW), bf16),
            jax.ShapeDtypeStruct((TOK, D), bf16),
        ),
        in_specs=[vmem] * 8 + [hbm] * 4,
        out_specs=(hbm, hbm),
        scratch_shapes=[
            buf(NC, TOK, C),
            buf(NC, NZ, BJ, C), buf(NC, NZ, BJ, C), buf(NC, NJ, BZ, C),
            buf(2, NC, NJ, BZ, C),
            buf(2, D, FL), buf(2, D, FL), buf(NC, 2 * FL, C),
            pltpu.VMEM((2, 4, S, FL), f32), buf(2, S, 2 * FL),
            buf(NC, S, C), buf(NC, S, C),
            buf(NC, NJ, BZ, C), buf(NC, NJ, BZ, C),
            buf(NC, NZ, BJ, C), buf(NC, NZ, BJ, C),
            buf(S, TOK), buf(TOK, S), buf(TOK, S),
            buf(4, TOK, GW), buf(HALO + 4 * TOK, GW), buf(GW, GW), buf(4 * TOK, GW),
            buf(NC, TOK, C),
            dma((4,)), dma((2,)), dma((11,)),
            dma((NC,)), dma((NC,)), dma((NC,)), dma((NC,)), dma((NC,)), dma((NC,)),
            dma((NC,)), dma((NC,)), dma((NC,)), dma((2,)),
        ],
        compiler_params=pltpu.CompilerParams(
            collective_id=0, has_side_effects=True, vmem_limit_bytes=67043328
        ),
        name="layer",
    )(
        expert_in, expert_gain[None], mixer_in, mixer_gain[None], routes.T, route_weight.T,
        group_scale, perm, group_weight, gate_weight, up_weight, down_weight,
    )


def solution(mesh):
    in_specs = (
        P(("ep", "tp"), None),
        P(),
        P("tp", None, None),
        P("tp", None),
        P(("ep", "tp"), None),
        P(),
        P("ep", None),
        P("ep", None),
        P("ep", None, "tp"),
        P("ep", None, "tp"),
        P("ep", "tp", None),
    )
    out_specs = (P("ep", "tp"), P(("ep", "tp"), None))
    return jax.shard_map(shards, mesh=mesh, in_specs=in_specs, out_specs=out_specs, check_vma=False)
```

```python
import functools

import jax
import jax.numpy as jnp
from jax import lax
from jax.experimental import pallas as pl
from jax.experimental.pallas import tpu as pltpu
from jax.sharding import PartitionSpec as P

WMAX = 16
TOP = 2
HALO = 128
epsilon = 1e-06
clamp_limit = 7.0
sigmoid_slope = 1.702
MESH = pl.DeviceIdType.MESH
f32 = jnp.float32
bf16 = jnp.bfloat16


def aligned(value, by):
    return pl.multiple_of(value, by)


def dot(a, b):
    return jnp.dot(a, b, preferred_element_type=f32)


def layer_kernel(
    dims,
    ein, egain, min_, mgain, routes, weights, scale, perm,
    gw_hbm, g_hbm, u_hbm, d_hbm,
    mixed_hbm, out_hbm,
    en, zsend, zrecv, ysend, xs, wg, wu, wd, acc, hid,
    psend, precv, rsend, rmid, rperm, rfin, pick, mix_hi, mix_lo,
    msend, ext, gw, mixed_buf, out_buf,
    lsem, osem, ssem, zr, yr, tr, wgr, wur, wdr, pr, rr, fr, mr,
):
    NZ, NJ, TOK, D, C, CAP, FL = dims
    NC = D // C
    E = NZ * NJ
    S = E * CAP
    BJ, BZ = NJ * CAP, NZ * CAP
    GW = D // 4
    ep = lax.axis_index("ep")
    t = lax.axis_index("tp")
    z = ep // NJ
    j = ep % NJ
    t_mate = t + 1 - 2 * (t % 2)
    w_mate = 3 - t

    def remote(src, dst, send, recv, e, tt):
        return pltpu.make_async_remote_copy(
            src_ref=src, dst_ref=dst, send_sem=send, recv_sem=recv,
            device_id=(e, tt), device_id_type=MESH,
        )

    def drain(src, dst, sem):
        pltpu.make_async_copy(src, dst, sem).wait()

    barrier = pltpu.get_barrier_semaphore()

    def hello(e, tt):
        pl.semaphore_signal(barrier, inc=1, device_id=(e, tt), device_id_type=MESH)

    lax.fori_loop(1, NZ, lambda k, _: (hello(((z + k) % NZ) * NJ + j, t), 0)[1], 0)
    lax.fori_loop(1, NJ, lambda k, _: (hello(z * NJ + (j + k) % NJ, t), 0)[1], 0)
    lax.fori_loop(1, 4, lambda k, _: (hello(ep, (t + k) % 4), 0)[1], 0)

    @pl.when(ep > 0)
    def _():
        hello(ep - 1, 3)

    own_g = pltpu.make_async_copy(g_hbm.at[0], wg.at[0], lsem.at[0])
    own_u = pltpu.make_async_copy(u_hbm.at[0], wu.at[0], lsem.at[1])
    own_w = pltpu.make_async_copy(gw_hbm.at[0], gw, lsem.at[3])
    own_g.start()
    own_u.start()
    own_w.start()

    def own_d(c):
        return pltpu.make_async_copy(
            d_hbm.at[0, :, pl.ds(aligned(c * C, C), C)], wd.at[c, pl.ds(0, FL)], lsem.at[2]
        )

    def start_own_d(c, _):
        own_d(c).start()
        return 0

    lax.fori_loop(0, NC, start_own_d, 0)

    def norm_rows(src, gain, i):
        rows = pl.ds(aligned(i * 16, 16), 16)
        values = src[rows, :].astype(f32)
        mean = jnp.mean(values * values, axis=-1, keepdims=True)
        return rows, (values * lax.rsqrt(mean + epsilon) * gain[...]).astype(bf16)

    def expert_rows(i, _):
        rows, values = norm_rows(ein, egain, i)
        for c in range(NC):
            en[c, rows, :] = values[:, c * C : (c + 1) * C]
        return 0

    lax.fori_loop(0, TOK // 16, expert_rows, 0)

    own = pl.ds(aligned(t * TOK, TOK), TOK)
    r0, r1 = routes[0:1, own], routes[1:2, own]
    w0, w1 = weights[0:1, own], weights[1:2, own]
    experts = lax.broadcasted_iota(jnp.int32, (E, TOK), 0)
    is0, is1 = experts == r0, experts == r1
    named = jnp.where(is0 | is1, 1.0, 0.0).astype(bf16)
    tri = jnp.where(
        lax.broadcasted_iota(jnp.int32, (TOK, TOK), 0)
        < lax.broadcasted_iota(jnp.int32, (TOK, TOK), 1),
        1.0,
        0.0,
    ).astype(bf16)
    earlier = dot(named, tri)
    rank0 = jnp.sum(jnp.where(is0, earlier, 0.0), axis=0, keepdims=True)
    rank1 = jnp.sum(jnp.where(is1, earlier, 0.0), axis=0, keepdims=True)
    slot0 = r0 * CAP + rank0.astype(jnp.int32)
    slot1 = r1 * CAP + rank1.astype(jnp.int32)
    slots = lax.broadcasted_iota(jnp.int32, (S, TOK), 0)
    at0, at1 = slots == slot0, slots == slot1
    pick[...] = jnp.where(at0 | at1, 1.0, 0.0).astype(bf16)
    share = (jnp.where(at0, w0, 0.0) + jnp.where(at1, w1, 0.0)).T
    high = share.astype(bf16)
    mix_hi[...] = high
    mix_lo[...] = (share - high.astype(f32)).astype(bf16)

    last = ((t + 1) // 4) * (1 - (ep + 1) // E)
    pl.semaphore_wait(barrier, (NZ - 1) + (NJ - 1) + 3 + 4 * last)

    def z_copy(c, k):
        there = (z + k) % NZ
        return remote(
            zsend.at[c, there], zrecv.at[c, z], ssem.at[0], zr.at[c], there * NJ + j, t
        )

    def start_z(c, _):
        zsend[c] = dot(pick[...], en[c]).astype(bf16).reshape(NZ, BJ, C)
        zrecv[c, z] = zsend[c, z]
        lax.fori_loop(1, NZ, lambda k, _: (z_copy(c, k).start(), 0)[1], 0)
        return 0

    def wg_copy(c):
        rows = pl.ds(aligned(c * C, C), C)
        return remote(g_hbm.at[0, rows], wg.at[1, rows], ssem.at[1], wgr.at[c], ep, w_mate)

    def wu_copy(c):
        rows = pl.ds(aligned(c * C, C), C)
        return remote(u_hbm.at[0, rows], wu.at[1, rows], ssem.at[2], wur.at[c], ep, w_mate)

    def wd_copy(c):
        return remote(
            d_hbm.at[0, :, pl.ds(aligned(c * C, C), C)], wd.at[c, pl.ds(FL, FL)],
            ssem.at[3], wdr.at[c], ep, w_mate,
        )

    def start_w(c, _):
        wg_copy(c).start()
        wu_copy(c).start()
        return 0

    start_z(0, 0)
    lax.fori_loop(0, NC, start_w, 0)
    lax.fori_loop(0, NC, lambda c, _: (wd_copy(c).start(), 0)[1], 0)
    lax.fori_loop(1, NC, start_z, 0)

    def mixer_rows(i, _):
        rows, values = norm_rows(min_, mgain, i)
        for g in range(4):
            msend[g, rows, :] = values[:, g * GW : (g + 1) * GW]
        return 0

    lax.fori_loop(0, TOK // 16, mixer_rows, 0)

    def m_copy(k):
        there = (t + k) % 4
        return remote(
            msend.at[there], ext.at[pl.ds(aligned(HALO + t * TOK, 16), TOK)],
            ssem.at[4], mr.at[0], ep, there,
        )

    def halo_copy(g):
        return remote(
            msend.at[g, pl.ds(TOK - WMAX, WMAX)], ext.at[pl.ds(HALO - WMAX, WMAX)],
            ssem.at[5], mr.at[1], ep + 1, g,
        )

    lax.fori_loop(1, 4, lambda k, _: (m_copy(k).start(), 0)[1], 0)
    ext[0 : HALO - WMAX] = jnp.zeros((HALO - WMAX, GW), bf16)
    ext[pl.ds(aligned(HALO + t * TOK, 16), TOK), :] = msend[t]

    @pl.when((t == 3) & (ep < E - 1))
    def _():
        lax.fori_loop(0, 4, lambda g, _: (halo_copy(g).start(), 0)[1], 0)

    @pl.when(ep == 0)
    def _():
        ext[HALO - WMAX : HALO] = jnp.zeros((WMAX, GW), bf16)

    def clear(k, _):
        acc[k // 4, k % 4] = jnp.zeros((S, FL), f32)
        return 0

    lax.fori_loop(0, 8, clear, 0)

    def y_copy(c, k):
        there = (j + k) % NJ
        return remote(
            ysend.at[c, there], xs.at[0, c, j], ssem.at[6], yr.at[c], z * NJ + there, t
        )

    def stage_y(c):
        drain(zsend.at[c, pl.ds(0, NZ - 1)], zrecv.at[c, pl.ds(0, NZ - 1)], zr.at[c])
        moved = dot(perm[...], zrecv[c].reshape(S, C)).astype(bf16)
        ysend[c] = moved.reshape(NJ, BZ, C)
        xs[0, c, j] = ysend[c, j]
        lax.fori_loop(1, NJ, lambda k, _: (y_copy(c, k).start(), 0)[1], 0)

    def t_copy(c):
        return remote(xs.at[0, c], xs.at[1, c], ssem.at[7], tr.at[c], ep, t_mate)

    def stage_t(c):
        drain(ysend.at[c, pl.ds(0, NJ - 1)], xs.at[0, c, pl.ds(0, NJ - 1)], yr.at[c])
        t_copy(c).start()

    def stage_in(c):
        t_copy(c).wait_recv()
        wg_copy(c).wait_recv()
        wu_copy(c).wait_recv()
        rows = pl.ds(aligned(c * C, C), C)

        def half(h, _):
            x = xs[h, c].reshape(S, C)
            for part in range(2):
                acc[h, part] += dot(x, wg[part, rows, :])
                acc[h, 2 + part] += dot(x, wu[part, rows, :])
            return 0

        lax.fori_loop(0, 2, half, 0)

    def mixer():
        own_w.wait()

        drain(msend.at[pl.ds(0, 3)], msend.at[pl.ds(0, 3)], mr.at[0])

        @pl.when(ep > 0)
        def _():
            drain(
                msend.at[0, pl.ds(0, WMAX)], ext.at[pl.ds(HALO - WMAX, WMAX)], mr.at[1]
            )

        window = jnp.left_shift(2, t)
        row = lax.broadcasted_iota(jnp.int32, (TOK, HALO + TOK), 0) + HALO
        col = lax.broadcasted_iota(jnp.int32, (TOK, HALO + TOK), 1)
        band = jnp.where((col <= row) & (col > row - window), 1.0, 0.0).astype(bf16)

        def block(b, _):
            start = aligned(b * TOK, TOK)
            sums = dot(band, ext[pl.ds(start, HALO + TOK), :])
            place = ep * (4 * TOK) + start + lax.broadcasted_iota(jnp.int32, (TOK, 1), 0)
            count = jnp.minimum(place + 1, window).astype(f32)
            center = ext[pl.ds(aligned(start + HALO, TOK), TOK), :].astype(f32)
            pooled = (sums / count - center).astype(bf16)
            mixed_buf[pl.ds(start, TOK), :] = (dot(pooled, gw[...]) * scale[...]).astype(bf16)
            return 0

        lax.fori_loop(0, 4, block, 0)
        pltpu.make_async_copy(mixed_buf, mixed_hbm, osem.at[0]).start()

    LAG = 3

    def step_in(i, _):
        @pl.when(i < NC)
        def _():
            stage_y(i)

        @pl.when(i == LAG)
        def _():
            own_g.wait()
            own_u.wait()

        @pl.when(i >= LAG)
        def _():
            stage_in(i - LAG)

        @pl.when(i < NC)
        def _():
            stage_t(i)

        return 0

    lax.fori_loop(0, NC + LAG, step_in, 0)

    def units(b, _):
        rows = pl.ds(aligned(b * 64, 64), 64)
        for h in range(2):
            for part in range(2):
                gate = jnp.minimum(acc[h, part, rows, :], clamp_limit)
                up = jnp.clip(acc[h, 2 + part, rows, :], -clamp_limit, clamp_limit)
                hid[h, rows, part * FL : (part + 1) * FL] = (
                    (up + 1.0) * gate * jax.nn.sigmoid(sigmoid_slope * gate)
                ).astype(bf16)
        return 0

    lax.fori_loop(0, S // 64, units, 0)

    def p_copy(c):
        return remote(psend.at[c], precv.at[c], ssem.at[8], pr.at[c], ep, t_mate)

    def stage_part(c):
        wd_copy(c).wait_recv()
        psend[c] = dot(hid[1], wd[c]).astype(bf16)
        p_copy(c).start()

    def r_copy(c, k):
        there = (j + k) % NJ
        return remote(
            rsend.at[c, there], rmid.at[c, j], ssem.at[9], rr.at[c], z * NJ + there, t
        )

    def stage_result(c):
        mine = dot(hid[0], wd[c])
        p_copy(c).wait_recv()
        rsend[c] = (mine + precv[c].astype(f32)).astype(bf16).reshape(NJ, BZ, C)
        rmid[c, j] = rsend[c, j]
        lax.fori_loop(1, NJ, lambda k, _: (r_copy(c, k).start(), 0)[1], 0)

    def f_copy(c, k):
        there = (z + k) % NZ
        return remote(
            rperm.at[c, there], rfin.at[c, z], ssem.at[10], fr.at[c], there * NJ + j, t
        )

    def stage_back(c):
        drain(rsend.at[c, pl.ds(0, NJ - 1)], rmid.at[c, pl.ds(0, NJ - 1)], rr.at[c])
        moved = dot(perm[...], rmid[c].reshape(S, C)).astype(bf16)
        rperm[c] = moved.reshape(NZ, BJ, C)
        rfin[c, z] = rperm[c, z]
        lax.fori_loop(1, NZ, lambda k, _: (f_copy(c, k).start(), 0)[1], 0)

    def out_copy(c):
        return pltpu.make_async_copy(
            out_buf.at[c], out_hbm.at[:, pl.ds(aligned(c * C, C), C)], osem.at[1]
        )

    def stage_out(c):
        drain(rperm.at[c, pl.ds(0, NZ - 1)], rfin.at[c, pl.ds(0, NZ - 1)], fr.at[c])
        rows = rfin[c].reshape(S, C)
        out_buf[c] = (dot(mix_hi[...], rows) + dot(mix_lo[...], rows)).astype(bf16)
        out_copy(c).start()

    lax.fori_loop(0, NC, lambda c, _: (own_d(c).wait(), 0)[1], 0)

    def step_out(i, _):
        @pl.when(i < NC)
        def _():
            stage_part(i)

        @pl.when((i >= 2) & (i < NC + 2))
        def _():
            stage_result(i - 2)

        @pl.when((i >= 3) & (i < NC + 3))
        def _():
            stage_back(i - 3)

        @pl.when(i == NC + 2)
        def _():
            mixer()

        @pl.when(i >= 5)
        def _():
            stage_out(i - 5)

        return 0

    lax.fori_loop(0, NC + 5, step_out, 0)

    drain(zsend.at[:, pl.ds(0, NZ - 1)], zrecv.at[:, pl.ds(0, NZ - 1)], ssem.at[0])
    drain(wg.at[1], wg.at[1], ssem.at[1])
    drain(wu.at[1], wu.at[1], ssem.at[2])
    drain(wd.at[:, pl.ds(FL, FL)], wd.at[:, pl.ds(FL, FL)], ssem.at[3])
    drain(msend.at[pl.ds(0, 3)], msend.at[pl.ds(0, 3)], ssem.at[4])

    @pl.when((t == 3) & (ep < E - 1))
    def _():
        drain(msend.at[:, pl.ds(0, WMAX)], msend.at[:, pl.ds(0, WMAX)], ssem.at[5])

    drain(ysend.at[:, pl.ds(0, NJ - 1)], ysend.at[:, pl.ds(0, NJ - 1)], ssem.at[6])
    drain(xs.at[0], xs.at[1], ssem.at[7])
    drain(psend, precv, ssem.at[8])
    drain(rsend.at[:, pl.ds(0, NJ - 1)], rsend.at[:, pl.ds(0, NJ - 1)], ssem.at[9])
    drain(rperm.at[:, pl.ds(0, NZ - 1)], rperm.at[:, pl.ds(0, NZ - 1)], ssem.at[10])
    pltpu.make_async_copy(mixed_buf, mixed_hbm, osem.at[0]).wait()
    lax.fori_loop(0, NC, lambda c, _: (out_copy(c).wait(), 0)[1], 0)


def shards(
    mixer_in, mixer_gain, group_weight, group_scale, expert_in, expert_gain,
    routes, route_weight, gate_weight, up_weight, down_weight,
):
    E = lax.axis_size("ep")
    NJ = 8 if E == 64 else 2
    NZ = E // NJ
    TOK, D = expert_in.shape
    CAP = max(2, 3 * TOK * TOP // (2 * E))
    S = E * CAP
    FL = gate_weight.shape[2]
    NC = 8 if D >= 4096 else 4
    C = D // NC
    GW = D // 4
    BJ, BZ = NJ * CAP, NZ * CAP
    index = jnp.arange(S, dtype=jnp.int32)
    swapped = (index // CAP % NJ) * BZ + (index // BJ) * CAP + index % CAP
    perm = (swapped[:, None] == index[None, :]).astype(bf16)
    vmem = pl.BlockSpec(memory_space=pltpu.VMEM)
    hbm = pl.BlockSpec(memory_space=pl.ANY)
    dma = pltpu.SemaphoreType.DMA
    buf = lambda *shape: pltpu.VMEM(shape, bf16)
    return pl.pallas_call(
        functools.partial(layer_kernel, (NZ, NJ, TOK, D, C, CAP, FL)),
        out_shape=(
            jax.ShapeDtypeStruct((4 * TOK, GW), bf16),
            jax.ShapeDtypeStruct((TOK, D), bf16),
        ),
        in_specs=[vmem] * 8 + [hbm] * 4,
        out_specs=(hbm, hbm),
        scratch_shapes=[
            buf(NC, TOK, C),
            buf(NC, NZ, BJ, C), buf(NC, NZ, BJ, C), buf(NC, NJ, BZ, C),
            buf(2, NC, NJ, BZ, C),
            buf(2, D, FL), buf(2, D, FL), buf(NC, 2 * FL, C),
            pltpu.VMEM((2, 4, S, FL), f32), buf(2, S, 2 * FL),
            buf(NC, S, C), buf(NC, S, C),
            buf(NC, NJ, BZ, C), buf(NC, NJ, BZ, C),
            buf(NC, NZ, BJ, C), buf(NC, NZ, BJ, C),
            buf(S, TOK), buf(TOK, S), buf(TOK, S),
            buf(4, TOK, GW), buf(HALO + 4 * TOK, GW), buf(GW, GW), buf(4 * TOK, GW),
            buf(NC, TOK, C),
            dma((4,)), dma((2,)), dma((11,)),
            dma((NC,)), dma((NC,)), dma((NC,)), dma((NC,)), dma((NC,)), dma((NC,)),
            dma((NC,)), dma((NC,)), dma((NC,)), dma((2,)),
        ],
        compiler_params=pltpu.CompilerParams(
            collective_id=0, has_side_effects=True, vmem_limit_bytes=67043328
        ),
        name="layer",
    )(
        expert_in, expert_gain[None], mixer_in, mixer_gain[None], routes.T, route_weight.T,
        group_scale, perm, group_weight, gate_weight, up_weight, down_weight,
    )


def solution(mesh):
    in_specs = (
        P(("ep", "tp"), None),
        P(),
        P("tp", None, None),
        P("tp", None),
        P(("ep", "tp"), None),
        P(),
        P("ep", None),
        P("ep", None),
        P("ep", None, "tp"),
        P("ep", None, "tp"),
        P("ep", "tp", None),
    )
    out_specs = (P("ep", "tp"), P(("ep", "tp"), None))
    return jax.shard_map(shards, mesh=mesh, in_specs=in_specs, out_specs=out_specs, check_vma=False)
```

```python
import functools

import jax
import jax.numpy as jnp
from jax import lax
from jax.experimental import pallas as pl
from jax.experimental.pallas import tpu as pltpu
from jax.sharding import PartitionSpec as P

WMAX = 16
TOP = 2
HALO = 128
epsilon = 1e-06
clamp_limit = 7.0
sigmoid_slope = 1.702
MESH = pl.DeviceIdType.MESH
f32 = jnp.float32
bf16 = jnp.bfloat16


def aligned(value, by):
    return pl.multiple_of(value, by)


def dot(a, b):
    return jnp.dot(a, b, preferred_element_type=f32)


def layer_kernel(
    dims,
    egain, mgain, routes, weights, scale,
    ein_hbm, min_hbm, gw_hbm, g_hbm, u_hbm, d_hbm,
    mixed_hbm, out_hbm,
    en, zsend, zrecv, ysend, xs, wg, wu, wd, acc, hid,
    psend, precv, rsend, rmid, rperm, rfin, pick, mix_hi, mix_lo,
    ein, min_, perm, msend, relay, ext, gw, mixed_buf, out_buf,
    lsem, osem, ssem, zr, yr, tr, wgr, wur, wdr, pr, rr, fr, mr,
):
    NZ, NJ, TOK, D, C, CAP, FL = dims
    NC = D // C
    E = NZ * NJ
    S = E * CAP
    BJ, BZ = NJ * CAP, NZ * CAP
    GW = D // 4
    ep = lax.axis_index("ep")
    t = lax.axis_index("tp")
    z = ep // NJ
    j = ep % NJ
    t_mate = t + 1 - 2 * (t % 2)
    w_mate = 3 - t

    def remote(src, dst, send, recv, e, tt):
        return pltpu.make_async_remote_copy(
            src_ref=src, dst_ref=dst, send_sem=send, recv_sem=recv,
            device_id=(e, tt), device_id_type=MESH,
        )

    def drain(src, dst, sem):
        pltpu.make_async_copy(src, dst, sem).wait()

    barrier = pltpu.get_barrier_semaphore()

    def hello(e, tt):
        pl.semaphore_signal(barrier, inc=1, device_id=(e, tt), device_id_type=MESH)

    lax.fori_loop(1, NZ, lambda k, _: (hello(((z + k) % NZ) * NJ + j, t), 0)[1], 0)
    lax.fori_loop(1, NJ, lambda k, _: (hello(z * NJ + (j + k) % NJ, t), 0)[1], 0)
    lax.fori_loop(1, 4, lambda k, _: (hello(ep, (t + k) % 4), 0)[1], 0)

    @pl.when(ep > 0)
    def _():
        hello(ep - 1, 3)

    own_g = pltpu.make_async_copy(g_hbm.at[0], wg.at[0], lsem.at[0])
    own_u = pltpu.make_async_copy(u_hbm.at[0], wu.at[0], lsem.at[1])
    own_w = pltpu.make_async_copy(gw_hbm.at[0], gw, lsem.at[3])
    own_e = pltpu.make_async_copy(ein_hbm, ein, lsem.at[5])
    own_e.start()
    own_m = pltpu.make_async_copy(min_hbm, min_, lsem.at[4])
    own_m.start()
    own_g.start()
    own_u.start()
    own_w.start()

    def own_d(c):
        return pltpu.make_async_copy(
            d_hbm.at[0, :, pl.ds(aligned(c * C, C), C)], wd.at[c, pl.ds(0, FL)], lsem.at[2]
        )

    def start_own_d(c, _):
        own_d(c).start()
        return 0

    lax.fori_loop(0, NC, start_own_d, 0)

    own = pl.ds(aligned(t * TOK, TOK), TOK)
    r0, r1 = routes[0:1, own], routes[1:2, own]
    w0, w1 = weights[0:1, own], weights[1:2, own]
    experts = lax.broadcasted_iota(jnp.int32, (E, TOK), 0)
    is0, is1 = experts == r0, experts == r1
    named = jnp.where(is0 | is1, 1.0, 0.0).astype(bf16)
    tri = jnp.where(
        lax.broadcasted_iota(jnp.int32, (TOK, TOK), 0)
        < lax.broadcasted_iota(jnp.int32, (TOK, TOK), 1),
        1.0,
        0.0,
    ).astype(bf16)
    earlier = dot(named, tri)
    rank0 = jnp.sum(jnp.where(is0, earlier, 0.0), axis=0, keepdims=True)
    rank1 = jnp.sum(jnp.where(is1, earlier, 0.0), axis=0, keepdims=True)
    slot0 = r0 * CAP + rank0.astype(jnp.int32)
    slot1 = r1 * CAP + rank1.astype(jnp.int32)
    slots = lax.broadcasted_iota(jnp.int32, (S, TOK), 0)
    at0, at1 = slots == slot0, slots == slot1
    pick[...] = jnp.where(at0 | at1, 1.0, 0.0).astype(bf16)
    share = (jnp.where(at0, w0, 0.0) + jnp.where(at1, w1, 0.0)).T
    high = share.astype(bf16)
    mix_hi[...] = high
    mix_lo[...] = (share - high.astype(f32)).astype(bf16)

    row = lax.broadcasted_iota(jnp.int32, (S, 1), 0).astype(f32)
    major = jnp.floor((row + 0.5) * (1.0 / BJ))
    rest = row - BJ * major
    minor = jnp.floor((rest + 0.5) * (1.0 / CAP))
    source = BZ * minor + CAP * major + (rest - CAP * minor)
    column = lax.broadcasted_iota(jnp.int32, (S, S), 1).astype(f32)
    perm[...] = jnp.where(column == source, 1.0, 0.0).astype(bf16)

    def norm_rows(src, gain, i):
        rows = pl.ds(aligned(i * 16, 16), 16)
        values = src[rows, :].astype(f32)
        mean = jnp.mean(values * values, axis=-1, keepdims=True)
        return rows, (values * lax.rsqrt(mean + epsilon) * gain[...]).astype(bf16)

    def expert_rows(i, _):
        rows, values = norm_rows(ein, egain, i)
        for c in range(NC):
            en[c, rows, :] = values[:, c * C : (c + 1) * C]
        return 0

    own_e.wait()
    lax.fori_loop(0, TOK // 16, expert_rows, 0)

    own_m.wait()
    def mixer_rows(i, _):
        rows, values = norm_rows(min_, mgain, i)
        for g in range(4):
            msend[g, rows, :] = values[:, g * GW : (g + 1) * GW]
        return 0

    lax.fori_loop(0, TOK // 16, mixer_rows, 0)

    last = ((t + 1) // 4) * (1 - (ep + 1) // E)
    pl.semaphore_wait(barrier, (NZ - 1) + (NJ - 1) + 3 + 4 * last)

    def z_copy(c, k):
        there = (z + k) % NZ
        return remote(
            zsend.at[c, there], zrecv.at[c, z], ssem.at[0], zr.at[c], there * NJ + j, t
        )

    def start_z(c, _):
        zsend[c] = dot(pick[...], en[c]).astype(bf16).reshape(NZ, BJ, C)
        zrecv[c, z] = zsend[c, z]
        lax.fori_loop(1, NZ, lambda k, _: (z_copy(c, k).start(), 0)[1], 0)
        return 0

    def wg_copy(c):
        rows = pl.ds(aligned(c * C, C), C)
        return remote(g_hbm.at[0, rows], wg.at[1, rows], ssem.at[1], wgr.at[c], ep, w_mate)

    def wu_copy(c):
        rows = pl.ds(aligned(c * C, C), C)
        return remote(u_hbm.at[0, rows], wu.at[1, rows], ssem.at[2], wur.at[c], ep, w_mate)

    def wd_copy(c):
        return remote(
            d_hbm.at[0, :, pl.ds(aligned(c * C, C), C)], wd.at[c, pl.ds(FL, FL)],
            ssem.at[3], wdr.at[c], ep, w_mate,
        )

    def start_w(c, _):
        wg_copy(c).start()
        wu_copy(c).start()
        return 0

    start_z(0, 0)
    lax.fori_loop(0, NC, start_w, 0)
    lax.fori_loop(0, NC, lambda c, _: (wd_copy(c).start(), 0)[1], 0)

    def m_rows(owner):
        return ext.at[pl.ds(aligned(HALO + owner * TOK, 16), TOK)]

    m_mate = remote(msend.at[t_mate], m_rows(t), ssem.at[4], mr.at[0], ep, t_mate)
    m_relay = remote(msend.at[3 - t_mate], relay, ssem.at[11], mr.at[2], ep, t_mate)
    m_weight = remote(msend.at[w_mate], m_rows(t), ssem.at[12], mr.at[3], ep, w_mate)
    m_passed = remote(relay, m_rows(t_mate), ssem.at[13], mr.at[4], ep, w_mate)

    def halo_copy(g):
        return remote(
            msend.at[g, pl.ds(TOK - WMAX, WMAX)], ext.at[pl.ds(HALO - WMAX, WMAX)],
            ssem.at[5], mr.at[1], ep + 1, g,
        )

    m_mate.start()
    m_relay.start()
    ext[0 : HALO - WMAX] = jnp.zeros((HALO - WMAX, GW), bf16)
    ext[pl.ds(aligned(HALO + t * TOK, 16), TOK), :] = msend[t]

    @pl.when((t == 3) & (ep < E - 1))
    def _():
        lax.fori_loop(0, 4, lambda g, _: (halo_copy(g).start(), 0)[1], 0)

    @pl.when(ep == 0)
    def _():
        ext[HALO - WMAX : HALO] = jnp.zeros((WMAX, GW), bf16)

    lax.fori_loop(1, NC, start_z, 0)

    def clear(k, _):
        acc[k // 4, k % 4] = jnp.zeros((S, FL), f32)
        return 0

    lax.fori_loop(0, 8, clear, 0)

    def y_copy(c, k):
        there = (j + k) % NJ
        return remote(
            ysend.at[c, there], xs.at[0, c, j], ssem.at[6], yr.at[c], z * NJ + there, t
        )

    def stage_y(c):
        drain(zsend.at[c, pl.ds(0, NZ - 1)], zrecv.at[c, pl.ds(0, NZ - 1)], zr.at[c])
        moved = dot(perm[...], zrecv[c].reshape(S, C)).astype(bf16)
        ysend[c] = moved.reshape(NJ, BZ, C)
        xs[0, c, j] = ysend[c, j]
        lax.fori_loop(1, NJ, lambda k, _: (y_copy(c, k).start(), 0)[1], 0)

    def t_copy(c):
        return remote(xs.at[0, c], xs.at[1, c], ssem.at[7], tr.at[c], ep, t_mate)

    def stage_t(c):
        drain(ysend.at[c, pl.ds(0, NJ - 1)], xs.at[0, c, pl.ds(0, NJ - 1)], yr.at[c])
        t_copy(c).start()

    def stage_in(c):
        t_copy(c).wait_recv()
        wg_copy(c).wait_recv()
        wu_copy(c).wait_recv()
        rows = pl.ds(aligned(c * C, C), C)

        def half(h, _):
            x = xs[h, c].reshape(S, C)
            for part in range(2):
                acc[h, part] += dot(x, wg[part, rows, :])
                acc[h, 2 + part] += dot(x, wu[part, rows, :])
            return 0

        lax.fori_loop(0, 2, half, 0)

    def mixer_wait():
        own_w.wait()
        m_mate.wait_recv()
        m_weight.wait_recv()
        m_passed.wait_recv()

        @pl.when(ep > 0)
        def _():
            drain(
                msend.at[0, pl.ds(0, WMAX)], ext.at[pl.ds(HALO - WMAX, WMAX)], mr.at[1]
            )

    def mixer_block(b):
        window = jnp.left_shift(2, t)
        row = lax.broadcasted_iota(jnp.int32, (TOK, HALO + TOK), 0) + HALO
        col = lax.broadcasted_iota(jnp.int32, (TOK, HALO + TOK), 1)
        band = jnp.where((col <= row) & (col > row - window), 1.0, 0.0).astype(bf16)
        start = aligned(b * TOK, TOK)
        sums = dot(band, ext[pl.ds(start, HALO + TOK), :])
        place = ep * (4 * TOK) + start + lax.broadcasted_iota(jnp.int32, (TOK, 1), 0)
        count = jnp.minimum(place + 1, window).astype(f32)
        center = ext[pl.ds(aligned(start + HALO, TOK), TOK), :].astype(f32)
        pooled = (sums / count - center).astype(bf16)
        mixed_buf[pl.ds(start, TOK), :] = (dot(pooled, gw[...]) * scale[...]).astype(bf16)
        mixed_copy(b).start()

    def mixed_copy(b):
        rows = pl.ds(aligned(b * TOK, TOK), TOK)
        return pltpu.make_async_copy(mixed_buf.at[rows], mixed_hbm.at[rows], osem.at[0])

    LAG = 4

    def step_in(i, _):
        @pl.when(i < NC)
        def _():
            stage_y(i)

        @pl.when((i >= 1) & (i < NC + 1))
        def _():
            stage_t(i - 1)

        @pl.when(i == LAG)
        def _():
            m_relay.wait_recv()
            m_passed.start()
            m_weight.start()
            own_g.wait()
            own_u.wait()

        @pl.when(i >= LAG)
        def _():
            stage_in(i - LAG)

        return 0

    lax.fori_loop(0, NC + LAG, step_in, 0)

    def units(b, _):
        rows = pl.ds(aligned(b * 64, 64), 64)
        for h in range(2):
            for part in range(2):
                gate = jnp.minimum(acc[h, part, rows, :], clamp_limit)
                up = jnp.clip(acc[h, 2 + part, rows, :], -clamp_limit, clamp_limit)
                hid[h, rows, part * FL : (part + 1) * FL] = (
                    (up + 1.0) * gate * jax.nn.sigmoid(sigmoid_slope * gate)
                ).astype(bf16)
        return 0

    lax.fori_loop(0, S // 64, units, 0)

    def p_copy(c):
        return remote(psend.at[c], precv.at[c], ssem.at[8], pr.at[c], ep, t_mate)

    def stage_part(c):
        wd_copy(c).wait_recv()
        psend[c] = dot(hid[1], wd[c]).astype(bf16)
        p_copy(c).start()

    def r_copy(c, k):
        there = (j + k) % NJ
        return remote(
            rsend.at[c, there], rmid.at[c, j], ssem.at[9], rr.at[c], z * NJ + there, t
        )

    def stage_result(c):
        mine = dot(hid[0], wd[c])
        p_copy(c).wait_recv()
        rsend[c] = (mine + precv[c].astype(f32)).astype(bf16).reshape(NJ, BZ, C)
        rmid[c, j] = rsend[c, j]
        lax.fori_loop(1, NJ, lambda k, _: (r_copy(c, k).start(), 0)[1], 0)

    def f_copy(c, k):
        there = (z + k) % NZ
        return remote(
            rperm.at[c, there], rfin.at[c, z], ssem.at[10], fr.at[c], there * NJ + j, t
        )

    def stage_back(c):
        drain(rsend.at[c, pl.ds(0, NJ - 1)], rmid.at[c, pl.ds(0, NJ - 1)], rr.at[c])
        moved = dot(perm[...], rmid[c].reshape(S, C)).astype(bf16)
        rperm[c] = moved.reshape(NZ, BJ, C)
        rfin[c, z] = rperm[c, z]
        lax.fori_loop(1, NZ, lambda k, _: (f_copy(c, k).start(), 0)[1], 0)

    def out_copy(c):
        return pltpu.make_async_copy(
            out_buf.at[c], out_hbm.at[:, pl.ds(aligned(c * C, C), C)], osem.at[1]
        )

    def stage_out(c):
        drain(rperm.at[c, pl.ds(0, NZ - 1)], rfin.at[c, pl.ds(0, NZ - 1)], fr.at[c])
        rows = rfin[c].reshape(S, C)
        out_buf[c] = (dot(mix_hi[...], rows) + dot(mix_lo[...], rows)).astype(bf16)
        out_copy(c).start()

    lax.fori_loop(0, NC, lambda c, _: (own_d(c).wait(), 0)[1], 0)

    def step_out(i, _):
        @pl.when(i < NC)
        def _():
            stage_part(i)

        @pl.when((i >= 2) & (i < NC + 2))
        def _():
            stage_result(i - 2)

        @pl.when((i >= 3) & (i < NC + 3))
        def _():
            stage_back(i - 3)

        @pl.when(i == NC - 1)
        def _():
            mixer_wait()

        @pl.when((i >= NC - 1) & (i < NC + 3))
        def _():
            mixer_block(i - (NC - 1))

        @pl.when(i >= 6)
        def _():
            stage_out(i - 6)

        return 0

    lax.fori_loop(0, NC + 6, step_out, 0)

    drain(zsend.at[:, pl.ds(0, NZ - 1)], zrecv.at[:, pl.ds(0, NZ - 1)], ssem.at[0])
    drain(wg.at[1], wg.at[1], ssem.at[1])
    drain(wu.at[1], wu.at[1], ssem.at[2])
    drain(wd.at[:, pl.ds(FL, FL)], wd.at[:, pl.ds(FL, FL)], ssem.at[3])
    m_mate.wait_send()
    m_relay.wait_send()
    m_weight.wait_send()
    m_passed.wait_send()

    @pl.when((t == 3) & (ep < E - 1))
    def _():
        drain(msend.at[:, pl.ds(0, WMAX)], msend.at[:, pl.ds(0, WMAX)], ssem.at[5])

    drain(ysend.at[:, pl.ds(0, NJ - 1)], ysend.at[:, pl.ds(0, NJ - 1)], ssem.at[6])
    drain(xs.at[0], xs.at[1], ssem.at[7])
    drain(psend, precv, ssem.at[8])
    drain(rsend.at[:, pl.ds(0, NJ - 1)], rsend.at[:, pl.ds(0, NJ - 1)], ssem.at[9])
    drain(rperm.at[:, pl.ds(0, NZ - 1)], rperm.at[:, pl.ds(0, NZ - 1)], ssem.at[10])
    lax.fori_loop(0, 4, lambda b, _: (mixed_copy(b).wait(), 0)[1], 0)
    lax.fori_loop(0, NC, lambda c, _: (out_copy(c).wait(), 0)[1], 0)


def shards(
    mixer_in, mixer_gain, group_weight, group_scale, expert_in, expert_gain,
    routes, route_weight, gate_weight, up_weight, down_weight,
):
    E = lax.axis_size("ep")
    NJ = 8 if E == 64 else 2
    NZ = E // NJ
    TOK, D = expert_in.shape
    CAP = max(2, 3 * TOK * TOP // (2 * E))
    S = E * CAP
    FL = gate_weight.shape[2]
    NC = 16 if D >= 4096 else 4
    C = D // NC
    GW = D // 4
    BJ, BZ = NJ * CAP, NZ * CAP
    vmem = pl.BlockSpec(memory_space=pltpu.VMEM)
    hbm = pl.BlockSpec(memory_space=pl.ANY)
    dma = pltpu.SemaphoreType.DMA
    buf = lambda *shape: pltpu.VMEM(shape, bf16)
    return pl.pallas_call(
        functools.partial(layer_kernel, (NZ, NJ, TOK, D, C, CAP, FL)),
        out_shape=(
            jax.ShapeDtypeStruct((4 * TOK, GW), bf16),
            jax.ShapeDtypeStruct((TOK, D), bf16),
        ),
        in_specs=[vmem] * 5 + [hbm] * 6,
        out_specs=(hbm, hbm),
        scratch_shapes=[
            buf(NC, TOK, C),
            buf(NC, NZ, BJ, C), buf(NC, NZ, BJ, C), buf(NC, NJ, BZ, C),
            buf(2, NC, NJ, BZ, C),
            buf(2, D, FL), buf(2, D, FL), buf(NC, 2 * FL, C),
            pltpu.VMEM((2, 4, S, FL), f32), buf(2, S, 2 * FL),
            buf(NC, S, C), buf(NC, S, C),
            buf(NC, NJ, BZ, C), buf(NC, NJ, BZ, C),
            buf(NC, NZ, BJ, C), buf(NC, NZ, BJ, C),
            buf(S, TOK), buf(TOK, S), buf(TOK, S),
            buf(TOK, D), buf(TOK, D), buf(S, S), buf(4, TOK, GW), buf(TOK, GW), buf(HALO + 4 * TOK, GW), buf(GW, GW), buf(4 * TOK, GW),
            buf(NC, TOK, C),
            dma((6,)), dma((2,)), dma((14,)),
            dma((NC,)), dma((NC,)), dma((NC,)), dma((NC,)), dma((NC,)), dma((NC,)),
            dma((NC,)), dma((NC,)), dma((NC,)), dma((5,)),
        ],
        compiler_params=pltpu.CompilerParams(
            collective_id=0, has_side_effects=True, vmem_limit_bytes=67043328
        ),
        name="layer",
    )(
        expert_gain[None], mixer_gain[None], routes.T, route_weight.T,
        group_scale, expert_in, mixer_in, group_weight, gate_weight, up_weight, down_weight,
    )


def solution(mesh):
    in_specs = (
        P(("ep", "tp"), None),
        P(),
        P("tp", None, None),
        P("tp", None),
        P(("ep", "tp"), None),
        P(),
        P("ep", None),
        P("ep", None),
        P("ep", None, "tp"),
        P("ep", None, "tp"),
        P("ep", "tp", None),
    )
    out_specs = (P("ep", "tp"), P(("ep", "tp"), None))
    return jax.shard_map(shards, mesh=mesh, in_specs=in_specs, out_specs=out_specs, check_vma=False)
```

```python
import functools

import jax
import jax.numpy as jnp
from jax import lax
from jax.experimental import pallas as pl
from jax.experimental.pallas import tpu as pltpu
from jax.sharding import PartitionSpec as P

WMAX = 16
TOP = 2
HALO = 128
CH2 = 32
LAGS = (3, 5, 9)
epsilon = 1e-06
clamp_limit = 7.0
sigmoid_slope = 1.702
MESH = pl.DeviceIdType.MESH
f32 = jnp.float32
bf16 = jnp.bfloat16


def aligned(value, by):
    return pl.multiple_of(value, by)


def dot(a, b):
    return jnp.dot(a, b, preferred_element_type=f32)


def layer_kernel(
    dims,
    egain, mgain, routes, weights, scale,
    ein_hbm, min_hbm, gw_hbm, g_hbm, u_hbm, d_hbm,
    mixed_hbm, out_hbm,
    en, zsend, zrecv, ysend, xs, wg, wu, wd, acc, hid,
    psend, precv, rsend, rmid, rperm, rfin, pick, mix_hi, mix_lo,
    ein, min_, perm, msend, relay, ext, gw, mixed_buf, out_buf,
    lsem, osem, ssem, zr, yr, tr, wgr, wur, wdr, pr, rr, fr, mr,
):
    NZ, NJ, TOK, D, C, C2, CAP, FL = dims
    NC, NC2 = D // C, D // C2
    E = NZ * NJ
    S = E * CAP
    BJ, BZ = NJ * CAP, NZ * CAP
    GW = D // 4
    ep = lax.axis_index("ep")
    t = lax.axis_index("tp")
    z = ep // NJ
    j = ep % NJ
    t_mate = t + 1 - 2 * (t % 2)
    w_mate = 3 - t

    def remote(src, dst, send, recv, e, tt):
        return pltpu.make_async_remote_copy(
            src_ref=src, dst_ref=dst, send_sem=send, recv_sem=recv,
            device_id=(e, tt), device_id_type=MESH,
        )

    def far(k, count):
        return count // 2 + (2 * (k % 2) - 1) * (k // 2)

    def drain(src, dst, sem):
        pltpu.make_async_copy(src, dst, sem).wait()

    barrier = pltpu.get_barrier_semaphore()

    def hello(e, tt):
        pl.semaphore_signal(barrier, inc=1, device_id=(e, tt), device_id_type=MESH)

    lax.fori_loop(1, NZ, lambda k, _: (hello(((z + k) % NZ) * NJ + j, t), 0)[1], 0)
    lax.fori_loop(1, NJ, lambda k, _: (hello(z * NJ + (j + k) % NJ, t), 0)[1], 0)
    lax.fori_loop(1, 4, lambda k, _: (hello(ep, (t + k) % 4), 0)[1], 0)

    @pl.when(ep > 0)
    def _():
        hello(ep - 1, 3)

    own_g = pltpu.make_async_copy(g_hbm.at[0], wg.at[0], lsem.at[0])
    own_u = pltpu.make_async_copy(u_hbm.at[0], wu.at[0], lsem.at[1])
    own_w = pltpu.make_async_copy(gw_hbm.at[0], gw, lsem.at[3])
    own_e = pltpu.make_async_copy(ein_hbm, ein, lsem.at[5])
    own_e.start()
    own_m = pltpu.make_async_copy(min_hbm, min_, lsem.at[4])
    own_m.start()
    own_g.start()
    own_u.start()
    own_w.start()

    def own_d(c):
        return pltpu.make_async_copy(
            d_hbm.at[0, :, pl.ds(aligned(c * C2, C2), C2)], wd.at[c, pl.ds(0, FL)], lsem.at[2]
        )

    def start_own_d(c, _):
        own_d(c).start()
        return 0

    lax.fori_loop(0, NC2, start_own_d, 0)

    own = pl.ds(aligned(t * TOK, TOK), TOK)
    r0, r1 = routes[0:1, own], routes[1:2, own]
    w0, w1 = weights[0:1, own], weights[1:2, own]
    experts = lax.broadcasted_iota(jnp.int32, (E, TOK), 0)
    is0, is1 = experts == r0, experts == r1
    named = jnp.where(is0 | is1, 1.0, 0.0).astype(bf16)
    tri = jnp.where(
        lax.broadcasted_iota(jnp.int32, (TOK, TOK), 0)
        < lax.broadcasted_iota(jnp.int32, (TOK, TOK), 1),
        1.0,
        0.0,
    ).astype(bf16)
    earlier = dot(named, tri)
    rank0 = jnp.sum(jnp.where(is0, earlier, 0.0), axis=0, keepdims=True)
    rank1 = jnp.sum(jnp.where(is1, earlier, 0.0), axis=0, keepdims=True)
    slot0 = r0 * CAP + rank0.astype(jnp.int32)
    slot1 = r1 * CAP + rank1.astype(jnp.int32)
    slots = lax.broadcasted_iota(jnp.int32, (S, TOK), 0)
    at0, at1 = slots == slot0, slots == slot1
    pick[...] = jnp.where(at0 | at1, 1.0, 0.0).astype(bf16)
    share = (jnp.where(at0, w0, 0.0) + jnp.where(at1, w1, 0.0)).T
    high = share.astype(bf16)
    mix_hi[...] = high
    mix_lo[...] = (share - high.astype(f32)).astype(bf16)

    row = lax.broadcasted_iota(jnp.int32, (S, 1), 0).astype(f32)
    major = jnp.floor((row + 0.5) * (1.0 / BJ))
    rest = row - BJ * major
    minor = jnp.floor((rest + 0.5) * (1.0 / CAP))
    source = BZ * minor + CAP * major + (rest - CAP * minor)
    column = lax.broadcasted_iota(jnp.int32, (S, S), 1).astype(f32)
    perm[...] = jnp.where(column == source, 1.0, 0.0).astype(bf16)

    last = ((t + 1) // 4) * (1 - (ep + 1) // E)
    pl.semaphore_wait(barrier, (NZ - 1) + (NJ - 1) + 3 + 4 * last)

    def z_copy(c, k):
        there = (z + far(k, NZ)) % NZ
        return remote(
            zsend.at[c, there], zrecv.at[c, z], ssem.at[0], zr.at[c], there * NJ + j, t
        )

    def start_z(c, _):
        zsend[c] = dot(pick[...], en[c]).astype(bf16).reshape(NZ, BJ, C)
        zrecv[c, z] = zsend[c, z]
        lax.fori_loop(1, NZ, lambda k, _: (z_copy(c, k).start(), 0)[1], 0)
        return 0

    def wg_copy(c):
        rows = pl.ds(aligned(c * C, C), C)
        return remote(g_hbm.at[0, rows], wg.at[1, rows], ssem.at[1], wgr.at[c], ep, w_mate)

    def wu_copy(c):
        rows = pl.ds(aligned(c * C, C), C)
        return remote(u_hbm.at[0, rows], wu.at[1, rows], ssem.at[2], wur.at[c], ep, w_mate)

    def wd_copy(c):
        return remote(
            d_hbm.at[0, :, pl.ds(aligned(c * C2, C2), C2)], wd.at[c, pl.ds(FL, FL)],
            ssem.at[3], wdr.at[c], ep, w_mate,
        )

    def start_w(c, _):
        wg_copy(c).start()
        wu_copy(c).start()
        return 0

    lax.fori_loop(0, NC, start_w, 0)
    lax.fori_loop(0, NC2, lambda c, _: (wd_copy(c).start(), 0)[1], 0)

    def norm_rows(src, gain, i):
        rows = pl.ds(aligned(i * 16, 16), 16)
        values = src[rows, :].astype(f32)
        mean = jnp.mean(values * values, axis=-1, keepdims=True)
        return rows, (values * lax.rsqrt(mean + epsilon) * gain[...]).astype(bf16)

    def expert_rows(i, _):
        rows, values = norm_rows(ein, egain, i)
        for c in range(NC):
            en[c, rows, :] = values[:, c * C : (c + 1) * C]
        return 0

    own_e.wait()
    lax.fori_loop(0, TOK // 16, expert_rows, 0)

    start_z(0, 0)
    start_z(1, 0)

    own_m.wait()
    def mixer_rows(i, _):
        rows, values = norm_rows(min_, mgain, i)
        for g in range(4):
            msend[g, rows, :] = values[:, g * GW : (g + 1) * GW]
        return 0

    lax.fori_loop(0, TOK // 16, mixer_rows, 0)

    def m_rows(owner):
        return ext.at[pl.ds(aligned(HALO + owner * TOK, 16), TOK)]

    m_mate = remote(msend.at[t_mate], m_rows(t), ssem.at[4], mr.at[0], ep, t_mate)
    m_relay = remote(msend.at[3 - t_mate], relay, ssem.at[11], mr.at[2], ep, t_mate)
    m_weight = remote(msend.at[w_mate], m_rows(t), ssem.at[12], mr.at[3], ep, w_mate)
    m_passed = remote(relay, m_rows(t_mate), ssem.at[13], mr.at[4], ep, w_mate)

    def halo_copy(g):
        return remote(
            msend.at[g, pl.ds(TOK - WMAX, WMAX)], ext.at[pl.ds(HALO - WMAX, WMAX)],
            ssem.at[5], mr.at[1], ep + 1, g,
        )

    m_mate.start()
    m_relay.start()
    ext[0 : HALO - WMAX] = jnp.zeros((HALO - WMAX, GW), bf16)
    ext[pl.ds(aligned(HALO + t * TOK, 16), TOK), :] = msend[t]

    @pl.when((t == 3) & (ep < E - 1))
    def _():
        lax.fori_loop(0, 4, lambda g, _: (halo_copy(g).start(), 0)[1], 0)

    @pl.when(ep == 0)
    def _():
        ext[HALO - WMAX : HALO] = jnp.zeros((WMAX, GW), bf16)

    lax.fori_loop(2, NC, start_z, 0)

    def clear(k, _):
        acc[k // 4, k % 4] = jnp.zeros((S, FL), f32)
        return 0

    lax.fori_loop(0, 8, clear, 0)

    def y_copy(c, k):
        there = (j + far(k, NJ)) % NJ
        return remote(
            ysend.at[c, there], xs.at[0, c, j], ssem.at[6], yr.at[c], z * NJ + there, t
        )

    def stage_y(c):
        drain(zsend.at[c, pl.ds(0, NZ - 1)], zrecv.at[c, pl.ds(0, NZ - 1)], zr.at[c])
        moved = dot(perm[...], zrecv[c].reshape(S, C)).astype(bf16)
        ysend[c] = moved.reshape(NJ, BZ, C)
        xs[0, c, j] = ysend[c, j]
        lax.fori_loop(1, NJ, lambda k, _: (y_copy(c, k).start(), 0)[1], 0)

    def t_copy(c):
        return remote(xs.at[0, c], xs.at[1, c], ssem.at[7], tr.at[c], ep, t_mate)

    def stage_t(c):
        drain(ysend.at[c, pl.ds(0, NJ - 1)], xs.at[0, c, pl.ds(0, NJ - 1)], yr.at[c])
        t_copy(c).start()

    def stage_in(c):
        t_copy(c).wait_recv()
        wg_copy(c).wait_recv()
        wu_copy(c).wait_recv()
        rows = pl.ds(aligned(c * C, C), C)

        def half(h, _):
            x = xs[h, c].reshape(S, C)
            for part in range(2):
                acc[h, part] += dot(x, wg[part, rows, :])
                acc[h, 2 + part] += dot(x, wu[part, rows, :])
            return 0

        lax.fori_loop(0, 2, half, 0)

    def mixer_wait():
        own_w.wait()
        m_mate.wait_recv()
        m_weight.wait_recv()
        m_passed.wait_recv()

        @pl.when(ep > 0)
        def _():
            drain(
                msend.at[0, pl.ds(0, WMAX)], ext.at[pl.ds(HALO - WMAX, WMAX)], mr.at[1]
            )

    def mixer_block(b):
        window = jnp.left_shift(2, t)
        row = lax.broadcasted_iota(jnp.int32, (TOK, HALO + TOK), 0) + HALO
        col = lax.broadcasted_iota(jnp.int32, (TOK, HALO + TOK), 1)
        band = jnp.where((col <= row) & (col > row - window), 1.0, 0.0).astype(bf16)
        start = aligned(b * TOK, TOK)
        sums = dot(band, ext[pl.ds(start, HALO + TOK), :])
        place = ep * (4 * TOK) + start + lax.broadcasted_iota(jnp.int32, (TOK, 1), 0)
        count = jnp.minimum(place + 1, window).astype(f32)
        center = ext[pl.ds(aligned(start + HALO, TOK), TOK), :].astype(f32)
        pooled = (sums / count - center).astype(bf16)
        mixed_buf[pl.ds(start, TOK), :] = (dot(pooled, gw[...]) * scale[...]).astype(bf16)
        mixed_copy(b).start()

    def mixed_copy(b):
        rows = pl.ds(aligned(b * TOK, TOK), TOK)
        return pltpu.make_async_copy(mixed_buf.at[rows], mixed_hbm.at[rows], osem.at[0])

    LAG = 4

    def step_in(i, _):
        @pl.when(i < NC)
        def _():
            stage_y(i)

        @pl.when((i >= 1) & (i < NC + 1))
        def _():
            stage_t(i - 1)

        @pl.when(i == LAG)
        def _():
            m_relay.wait_recv()
            m_passed.start()
            m_weight.start()
            own_g.wait()
            own_u.wait()

        @pl.when(i >= LAG)
        def _():
            stage_in(i - LAG)

        return 0

    lax.fori_loop(0, NC + LAG, step_in, 0)

    def units(b, _):
        rows = pl.ds(aligned(b * 64, 64), 64)
        for h in range(2):
            for part in range(2):
                gate = jnp.minimum(acc[h, part, rows, :], clamp_limit)
                up = jnp.clip(acc[h, 2 + part, rows, :], -clamp_limit, clamp_limit)
                hid[h, rows, part * FL : (part + 1) * FL] = (
                    (up + 1.0) * gate * jax.nn.sigmoid(sigmoid_slope * gate)
                ).astype(bf16)
        return 0

    lax.fori_loop(0, S // 64, units, 0)

    def p_copy(c):
        return remote(psend.at[c], precv.at[c], ssem.at[8], pr.at[c], ep, t_mate)

    def stage_part(c):
        wd_copy(c).wait_recv()
        psend[c] = dot(hid[1], wd[c]).astype(bf16)
        p_copy(c).start()

    def r_copy(c, k):
        there = (j + far(k, NJ)) % NJ
        return remote(
            rsend.at[c, there], rmid.at[c, j], ssem.at[9], rr.at[c], z * NJ + there, t
        )

    def stage_result(c):
        mine = dot(hid[0], wd[c])
        p_copy(c).wait_recv()
        rsend[c] = (mine + precv[c].astype(f32)).astype(bf16).reshape(NJ, BZ, C2)
        rmid[c, j] = rsend[c, j]
        lax.fori_loop(1, NJ, lambda k, _: (r_copy(c, k).start(), 0)[1], 0)

    def f_copy(c, k):
        there = (z + far(k, NZ)) % NZ
        return remote(
            rperm.at[c, there], rfin.at[c, z], ssem.at[10], fr.at[c], there * NJ + j, t
        )

    def stage_back(c):
        drain(rsend.at[c, pl.ds(0, NJ - 1)], rmid.at[c, pl.ds(0, NJ - 1)], rr.at[c])
        moved = dot(perm[...], rmid[c].reshape(S, C2)).astype(bf16)
        rperm[c] = moved.reshape(NZ, BJ, C2)
        rfin[c, z] = rperm[c, z]
        lax.fori_loop(1, NZ, lambda k, _: (f_copy(c, k).start(), 0)[1], 0)

    def out_copy(c):
        return pltpu.make_async_copy(
            out_buf.at[c], out_hbm.at[:, pl.ds(aligned(c * C2, C2), C2)], osem.at[1]
        )

    def stage_out(c):
        drain(rperm.at[c, pl.ds(0, NZ - 1)], rfin.at[c, pl.ds(0, NZ - 1)], fr.at[c])
        rows = rfin[c].reshape(S, C2)
        out_buf[c] = (dot(mix_hi[...], rows) + dot(mix_lo[...], rows)).astype(bf16)
        out_copy(c).start()

    lax.fori_loop(0, NC2, lambda c, _: (own_d(c).wait(), 0)[1], 0)

    A, B, O = LAGS

    def step_out(i, _):
        @pl.when(i < NC2)
        def _():
            stage_part(i)

        @pl.when((i >= A) & (i < NC2 + A))
        def _():
            stage_result(i - A)

        @pl.when((i >= B) & (i < NC2 + B))
        def _():
            stage_back(i - B)

        @pl.when(i == NC2 - 2)
        def _():
            mixer_wait()

        @pl.when((i >= NC2 - 2) & (i < NC2 + 2))
        def _():
            mixer_block(i - (NC2 - 2))

        @pl.when(i >= O)
        def _():
            stage_out(i - O)

        return 0

    lax.fori_loop(0, NC2 + O, step_out, 0)

    drain(zsend.at[:, pl.ds(0, NZ - 1)], zrecv.at[:, pl.ds(0, NZ - 1)], ssem.at[0])
    drain(wg.at[1], wg.at[1], ssem.at[1])
    drain(wu.at[1], wu.at[1], ssem.at[2])
    drain(wd.at[:, pl.ds(FL, FL)], wd.at[:, pl.ds(FL, FL)], ssem.at[3])
    m_mate.wait_send()
    m_relay.wait_send()
    m_weight.wait_send()
    m_passed.wait_send()

    @pl.when((t == 3) & (ep < E - 1))
    def _():
        drain(msend.at[:, pl.ds(0, WMAX)], msend.at[:, pl.ds(0, WMAX)], ssem.at[5])

    drain(ysend.at[:, pl.ds(0, NJ - 1)], ysend.at[:, pl.ds(0, NJ - 1)], ssem.at[6])
    drain(xs.at[0], xs.at[1], ssem.at[7])
    drain(psend, precv, ssem.at[8])
    drain(rsend.at[:, pl.ds(0, NJ - 1)], rsend.at[:, pl.ds(0, NJ - 1)], ssem.at[9])
    drain(rperm.at[:, pl.ds(0, NZ - 1)], rperm.at[:, pl.ds(0, NZ - 1)], ssem.at[10])
    lax.fori_loop(0, 4, lambda b, _: (mixed_copy(b).wait(), 0)[1], 0)
    lax.fori_loop(0, NC2, lambda c, _: (out_copy(c).wait(), 0)[1], 0)


def shards(
    mixer_in, mixer_gain, group_weight, group_scale, expert_in, expert_gain,
    routes, route_weight, gate_weight, up_weight, down_weight,
):
    E = lax.axis_size("ep")
    NJ = 8 if E == 64 else 2
    NZ = E // NJ
    TOK, D = expert_in.shape
    CAP = max(2, 3 * TOK * TOP // (2 * E))
    S = E * CAP
    FL = gate_weight.shape[2]
    NC = 16 if D >= 4096 else 4
    C = D // NC
    C2 = D // (CH2 if D >= 4096 else 4)
    NC2 = D // C2
    GW = D // 4
    BJ, BZ = NJ * CAP, NZ * CAP
    vmem = pl.BlockSpec(memory_space=pltpu.VMEM)
    hbm = pl.BlockSpec(memory_space=pl.ANY)
    dma = pltpu.SemaphoreType.DMA
    buf = lambda *shape: pltpu.VMEM(shape, bf16)
    return pl.pallas_call(
        functools.partial(layer_kernel, (NZ, NJ, TOK, D, C, C2, CAP, FL)),
        out_shape=(
            jax.ShapeDtypeStruct((4 * TOK, GW), bf16),
            jax.ShapeDtypeStruct((TOK, D), bf16),
        ),
        in_specs=[vmem] * 5 + [hbm] * 6,
        out_specs=(hbm, hbm),
        scratch_shapes=[
            buf(NC, TOK, C),
            buf(NC, NZ, BJ, C), buf(NC, NZ, BJ, C), buf(NC, NJ, BZ, C),
            buf(2, NC, NJ, BZ, C),
            buf(2, D, FL), buf(2, D, FL), buf(NC2, 2 * FL, C2),
            pltpu.VMEM((2, 4, S, FL), f32), buf(2, S, 2 * FL),
            buf(NC2, S, C2), buf(NC2, S, C2),
            buf(NC2, NJ, BZ, C2), buf(NC2, NJ, BZ, C2),
            buf(NC2, NZ, BJ, C2), buf(NC2, NZ, BJ, C2),
            buf(S, TOK), buf(TOK, S), buf(TOK, S),
            buf(TOK, D), buf(TOK, D), buf(S, S), buf(4, TOK, GW), buf(TOK, GW), buf(HALO + 4 * TOK, GW), buf(GW, GW), buf(4 * TOK, GW),
            buf(NC2, TOK, C2),
            dma((6,)), dma((2,)), dma((14,)),
            dma((NC,)), dma((NC,)), dma((NC,)), dma((NC,)), dma((NC,)), dma((NC2,)),
            dma((NC2,)), dma((NC2,)), dma((NC2,)), dma((5,)),
        ],
        compiler_params=pltpu.CompilerParams(
            collective_id=0, has_side_effects=True, vmem_limit_bytes=67043328
        ),
        name="layer",
    )(
        expert_gain[None], mixer_gain[None], routes.T, route_weight.T,
        group_scale, expert_in, mixer_in, group_weight, gate_weight, up_weight, down_weight,
    )


def solution(mesh):
    in_specs = (
        P(("ep", "tp"), None),
        P(),
        P("tp", None, None),
        P("tp", None),
        P(("ep", "tp"), None),
        P(),
        P("ep", None),
        P("ep", None),
        P("ep", None, "tp"),
        P("ep", None, "tp"),
        P("ep", "tp", None),
    )
    out_specs = (P("ep", "tp"), P(("ep", "tp"), None))
    return jax.shard_map(shards, mesh=mesh, in_specs=in_specs, out_specs=out_specs, check_vma=False)
```

```python
import functools

import jax
import jax.numpy as jnp
from jax import lax
from jax.experimental import pallas as pl
from jax.experimental.pallas import tpu as pltpu
from jax.sharding import PartitionSpec as P

WMAX = 16
TOP = 2
HALO = 128
CH2 = 32
LAGS = (3, 5, 9)
epsilon = 1e-06
clamp_limit = 7.0
sigmoid_slope = 1.702
MESH = pl.DeviceIdType.MESH
f32 = jnp.float32
bf16 = jnp.bfloat16


def aligned(value, by):
    return pl.multiple_of(value, by)


def dot(a, b):
    return jnp.dot(a, b, preferred_element_type=f32)


def layer_kernel(
    dims,
    egain_hbm, mgain_hbm, routes_hbm, weights_hbm, scale_hbm,
    ein_hbm, min_hbm, gw_hbm, g_hbm, u_hbm, d_hbm,
    mixed_hbm, out_hbm,
    en, zsend, zrecv, ysend, xs, wg, wu, wd, acc, hid,
    psend, precv, rsend, rmid, rperm, rfin, pick, mix_hi, mix_lo,
    egain, mgain, routes, weights, scale,
    ein, min_, perm, msend, relay, ext, gw, mixed_buf, out_buf,
    lsem, osem, ssem, zr, yr, tr, wgr, wur, wdr, pr, rr, fr, mr,
):
    NZ, NJ, TOK, D, C, C2, CAP, FL = dims
    NC, NC2 = D // C, D // C2
    E = NZ * NJ
    S = E * CAP
    BJ, BZ = NJ * CAP, NZ * CAP
    GW = D // 4
    ep = lax.axis_index("ep")
    t = lax.axis_index("tp")
    z = ep // NJ
    j = ep % NJ
    t_mate = t + 1 - 2 * (t % 2)
    w_mate = 3 - t

    def remote(src, dst, send, recv, e, tt):
        return pltpu.make_async_remote_copy(
            src_ref=src, dst_ref=dst, send_sem=send, recv_sem=recv,
            device_id=(e, tt), device_id_type=MESH,
        )

    def far(k, count):
        return count // 2 + (2 * (k % 2) - 1) * (k // 2)

    def drain(src, dst, sem):
        pltpu.make_async_copy(src, dst, sem).wait()

    barrier = pltpu.get_barrier_semaphore()

    def hello(e, tt):
        pl.semaphore_signal(barrier, inc=1, device_id=(e, tt), device_id_type=MESH)

    lax.fori_loop(1, NZ, lambda k, _: (hello(((z + k) % NZ) * NJ + j, t), 0)[1], 0)
    lax.fori_loop(1, NJ, lambda k, _: (hello(z * NJ + (j + k) % NJ, t), 0)[1], 0)
    lax.fori_loop(1, 4, lambda k, _: (hello(ep, (t + k) % 4), 0)[1], 0)

    @pl.when(ep > 0)
    def _():
        hello(ep - 1, 3)

    own_g = pltpu.make_async_copy(g_hbm.at[0], wg.at[0], lsem.at[0])
    own_u = pltpu.make_async_copy(u_hbm.at[0], wu.at[0], lsem.at[1])
    own_w = pltpu.make_async_copy(gw_hbm.at[0], gw, lsem.at[3])
    small = [
        pltpu.make_async_copy(a, b, lsem.at[6 + n])
        for n, (a, b) in enumerate(
            (
                (routes_hbm, routes), (weights_hbm, weights), (egain_hbm, egain),
                (mgain_hbm, mgain), (scale_hbm, scale),
            )
        )
    ]
    for copy in small:
        copy.start()
    own_e = pltpu.make_async_copy(ein_hbm, ein, lsem.at[5])
    own_e.start()
    own_m = pltpu.make_async_copy(min_hbm, min_, lsem.at[4])
    own_m.start()
    own_g.start()
    own_u.start()
    own_w.start()

    def own_d(c):
        return pltpu.make_async_copy(
            d_hbm.at[0, :, pl.ds(aligned(c * C2, C2), C2)], wd.at[c, pl.ds(0, FL)], lsem.at[2]
        )

    def start_own_d(c, _):
        own_d(c).start()
        return 0

    lax.fori_loop(0, NC2, start_own_d, 0)

    for copy in small:
        copy.wait()
    own = pl.ds(aligned(t * TOK, TOK), TOK)
    r0, r1 = routes[0:1, own], routes[1:2, own]
    w0, w1 = weights[0:1, own], weights[1:2, own]
    experts = lax.broadcasted_iota(jnp.int32, (E, TOK), 0)
    is0, is1 = experts == r0, experts == r1
    named = jnp.where(is0 | is1, 1.0, 0.0).astype(bf16)
    tri = jnp.where(
        lax.broadcasted_iota(jnp.int32, (TOK, TOK), 0)
        < lax.broadcasted_iota(jnp.int32, (TOK, TOK), 1),
        1.0,
        0.0,
    ).astype(bf16)
    earlier = dot(named, tri)
    rank0 = jnp.sum(jnp.where(is0, earlier, 0.0), axis=0, keepdims=True)
    rank1 = jnp.sum(jnp.where(is1, earlier, 0.0), axis=0, keepdims=True)
    slot0 = r0 * CAP + rank0.astype(jnp.int32)
    slot1 = r1 * CAP + rank1.astype(jnp.int32)
    slots = lax.broadcasted_iota(jnp.int32, (S, TOK), 0)
    at0, at1 = slots == slot0, slots == slot1
    pick[...] = jnp.where(at0 | at1, 1.0, 0.0).astype(bf16)
    share = (jnp.where(at0, w0, 0.0) + jnp.where(at1, w1, 0.0)).T
    high = share.astype(bf16)
    mix_hi[...] = high
    mix_lo[...] = (share - high.astype(f32)).astype(bf16)

    row = lax.broadcasted_iota(jnp.int32, (S, 1), 0).astype(f32)
    major = jnp.floor((row + 0.5) * (1.0 / BJ))
    rest = row - BJ * major
    minor = jnp.floor((rest + 0.5) * (1.0 / CAP))
    source = BZ * minor + CAP * major + (rest - CAP * minor)
    column = lax.broadcasted_iota(jnp.int32, (S, S), 1).astype(f32)
    perm[...] = jnp.where(column == source, 1.0, 0.0).astype(bf16)

    last = ((t + 1) // 4) * (1 - (ep + 1) // E)
    pl.semaphore_wait(barrier, (NZ - 1) + (NJ - 1) + 3 + 4 * last)

    def z_copy(c, k):
        there = (z + far(k, NZ)) % NZ
        return remote(
            zsend.at[c, there], zrecv.at[c, z], ssem.at[0], zr.at[c], there * NJ + j, t
        )

    def start_z(c, _):
        zsend[c] = dot(pick[...], en[c]).astype(bf16).reshape(NZ, BJ, C)
        zrecv[c, z] = zsend[c, z]
        lax.fori_loop(1, NZ, lambda k, _: (z_copy(c, k).start(), 0)[1], 0)
        return 0

    def wg_copy(c):
        rows = pl.ds(aligned(c * C, C), C)
        return remote(g_hbm.at[0, rows], wg.at[1, rows], ssem.at[1], wgr.at[c], ep, w_mate)

    def wu_copy(c):
        rows = pl.ds(aligned(c * C, C), C)
        return remote(u_hbm.at[0, rows], wu.at[1, rows], ssem.at[2], wur.at[c], ep, w_mate)

    def wd_copy(c):
        return remote(
            d_hbm.at[0, :, pl.ds(aligned(c * C2, C2), C2)], wd.at[c, pl.ds(FL, FL)],
            ssem.at[3], wdr.at[c], ep, w_mate,
        )

    def start_w(c, _):
        wg_copy(c).start()
        wu_copy(c).start()
        return 0

    lax.fori_loop(0, NC, start_w, 0)
    lax.fori_loop(0, NC2, lambda c, _: (wd_copy(c).start(), 0)[1], 0)

    def norm_rows(src, gain, i):
        rows = pl.ds(aligned(i * 16, 16), 16)
        values = src[rows, :].astype(f32)
        mean = jnp.mean(values * values, axis=-1, keepdims=True)
        return rows, (values * lax.rsqrt(mean + epsilon) * gain[...]).astype(bf16)

    def expert_rows(i, _):
        rows, values = norm_rows(ein, egain, i)
        for c in range(NC):
            en[c, rows, :] = values[:, c * C : (c + 1) * C]
        return 0

    own_e.wait()
    lax.fori_loop(0, TOK // 16, expert_rows, 0)

    start_z(0, 0)
    start_z(1, 0)

    own_m.wait()
    def mixer_rows(i, _):
        rows, values = norm_rows(min_, mgain, i)
        for g in range(4):
            msend[g, rows, :] = values[:, g * GW : (g + 1) * GW]
        return 0

    lax.fori_loop(0, TOK // 16, mixer_rows, 0)

    def m_rows(owner):
        return ext.at[pl.ds(aligned(HALO + owner * TOK, 16), TOK)]

    m_mate = remote(msend.at[t_mate], m_rows(t), ssem.at[4], mr.at[0], ep, t_mate)
    m_relay = remote(msend.at[3 - t_mate], relay, ssem.at[11], mr.at[2], ep, t_mate)
    m_weight = remote(msend.at[w_mate], m_rows(t), ssem.at[12], mr.at[3], ep, w_mate)
    m_passed = remote(relay, m_rows(t_mate), ssem.at[13], mr.at[4], ep, w_mate)

    def halo_copy(g):
        return remote(
            msend.at[g, pl.ds(TOK - WMAX, WMAX)], ext.at[pl.ds(HALO - WMAX, WMAX)],
            ssem.at[5], mr.at[1], ep + 1, g,
        )

    m_mate.start()
    m_relay.start()
    ext[0 : HALO - WMAX] = jnp.zeros((HALO - WMAX, GW), bf16)
    ext[pl.ds(aligned(HALO + t * TOK, 16), TOK), :] = msend[t]

    @pl.when((t == 3) & (ep < E - 1))
    def _():
        lax.fori_loop(0, 4, lambda g, _: (halo_copy(g).start(), 0)[1], 0)

    @pl.when(ep == 0)
    def _():
        ext[HALO - WMAX : HALO] = jnp.zeros((WMAX, GW), bf16)

    lax.fori_loop(2, NC, start_z, 0)

    def clear(k, _):
        acc[k // 4, k % 4] = jnp.zeros((S, FL), f32)
        return 0

    lax.fori_loop(0, 8, clear, 0)

    def y_copy(c, k):
        there = (j + far(k, NJ)) % NJ
        return remote(
            ysend.at[c, there], xs.at[0, c, j], ssem.at[6], yr.at[c], z * NJ + there, t
        )

    def stage_y(c):
        drain(zsend.at[c, pl.ds(0, NZ - 1)], zrecv.at[c, pl.ds(0, NZ - 1)], zr.at[c])
        moved = dot(perm[...], zrecv[c].reshape(S, C)).astype(bf16)
        ysend[c] = moved.reshape(NJ, BZ, C)
        xs[0, c, j] = ysend[c, j]
        lax.fori_loop(1, NJ, lambda k, _: (y_copy(c, k).start(), 0)[1], 0)

    def t_copy(c):
        return remote(xs.at[0, c], xs.at[1, c], ssem.at[7], tr.at[c], ep, t_mate)

    def stage_t(c):
        drain(ysend.at[c, pl.ds(0, NJ - 1)], xs.at[0, c, pl.ds(0, NJ - 1)], yr.at[c])
        t_copy(c).start()

    def wait_in(c):
        t_copy(c).wait_recv()
        wg_copy(c).wait_recv()
        wu_copy(c).wait_recv()

    def half_in(c, h):
        rows = pl.ds(aligned(c * C, C), C)
        x = xs[h, c].reshape(S, C)
        for part in range(2):
            acc[h, part] += dot(x, wg[part, rows, :])
            acc[h, 2 + part] += dot(x, wu[part, rows, :])

    def stage_in(c):
        wait_in(c)
        lax.fori_loop(0, 2, lambda h, _: (half_in(c, h), 0)[1], 0)

    def mixer_wait():
        own_w.wait()
        m_mate.wait_recv()
        m_weight.wait_recv()
        m_passed.wait_recv()

        @pl.when(ep > 0)
        def _():
            drain(
                msend.at[0, pl.ds(0, WMAX)], ext.at[pl.ds(HALO - WMAX, WMAX)], mr.at[1]
            )

    def mixer_block(b):
        window = jnp.left_shift(2, t)
        row = lax.broadcasted_iota(jnp.int32, (TOK, HALO + TOK), 0) + HALO
        col = lax.broadcasted_iota(jnp.int32, (TOK, HALO + TOK), 1)
        band = jnp.where((col <= row) & (col > row - window), 1.0, 0.0).astype(bf16)
        start = aligned(b * TOK, TOK)
        sums = dot(band, ext[pl.ds(start, HALO + TOK), :])
        place = ep * (4 * TOK) + start + lax.broadcasted_iota(jnp.int32, (TOK, 1), 0)
        count = jnp.minimum(place + 1, window).astype(f32)
        center = ext[pl.ds(aligned(start + HALO, TOK), TOK), :].astype(f32)
        pooled = (sums / count - center).astype(bf16)
        mixed_buf[pl.ds(start, TOK), :] = (dot(pooled, gw[...]) * scale[...]).astype(bf16)
        mixed_copy(b).start()

    def mixed_copy(b):
        rows = pl.ds(aligned(b * TOK, TOK), TOK)
        return pltpu.make_async_copy(mixed_buf.at[rows], mixed_hbm.at[rows], osem.at[0])

    LAG = 4

    def step_in(i, _):
        @pl.when(i < NC)
        def _():
            stage_y(i)

        @pl.when((i >= 1) & (i < NC + 1))
        def _():
            stage_t(i - 1)

        @pl.when(i == LAG)
        def _():
            m_relay.wait_recv()
            m_passed.start()
            m_weight.start()
            own_g.wait()
            own_u.wait()

        @pl.when(i >= LAG)
        def _():
            stage_in(i - LAG)

        return 0

    lax.fori_loop(0, NC + LAG - 1, step_in, 0)

    def units(h):
        def block(b, _):
            rows = pl.ds(aligned(b * 64, 64), 64)
            for part in range(2):
                gate = jnp.minimum(acc[h, part, rows, :], clamp_limit)
                up = jnp.clip(acc[h, 2 + part, rows, :], -clamp_limit, clamp_limit)
                hid[h, rows, part * FL : (part + 1) * FL] = (
                    (up + 1.0) * gate * jax.nn.sigmoid(sigmoid_slope * gate)
                ).astype(bf16)
            return 0

        lax.fori_loop(0, S // 64, block, 0)

    def p_copy(c):
        return remote(psend.at[c], precv.at[c], ssem.at[8], pr.at[c], ep, t_mate)

    def stage_part(c):
        wd_copy(c).wait_recv()
        psend[c] = dot(hid[1], wd[c]).astype(bf16)
        p_copy(c).start()

    def r_copy(c, k):
        there = (j + far(k, NJ)) % NJ
        return remote(
            rsend.at[c, there], rmid.at[c, j], ssem.at[9], rr.at[c], z * NJ + there, t
        )

    def stage_result(c):
        mine = dot(hid[0], wd[c])
        p_copy(c).wait_recv()
        rsend[c] = (mine + precv[c].astype(f32)).astype(bf16).reshape(NJ, BZ, C2)
        rmid[c, j] = rsend[c, j]
        lax.fori_loop(1, NJ, lambda k, _: (r_copy(c, k).start(), 0)[1], 0)

    def f_copy(c, k):
        there = (z + far(k, NZ)) % NZ
        return remote(
            rperm.at[c, there], rfin.at[c, z], ssem.at[10], fr.at[c], there * NJ + j, t
        )

    def stage_back(c):
        drain(rsend.at[c, pl.ds(0, NJ - 1)], rmid.at[c, pl.ds(0, NJ - 1)], rr.at[c])
        moved = dot(perm[...], rmid[c].reshape(S, C2)).astype(bf16)
        rperm[c] = moved.reshape(NZ, BJ, C2)
        rfin[c, z] = rperm[c, z]
        lax.fori_loop(1, NZ, lambda k, _: (f_copy(c, k).start(), 0)[1], 0)

    def out_copy(c):
        return pltpu.make_async_copy(
            out_buf.at[c], out_hbm.at[:, pl.ds(aligned(c * C2, C2), C2)], osem.at[1]
        )

    def stage_out(c):
        drain(rperm.at[c, pl.ds(0, NZ - 1)], rfin.at[c, pl.ds(0, NZ - 1)], fr.at[c])
        rows = rfin[c].reshape(S, C2)
        out_buf[c] = (dot(mix_hi[...], rows) + dot(mix_lo[...], rows)).astype(bf16)
        out_copy(c).start()

    lax.fori_loop(0, NC2, lambda c, _: (own_d(c).wait(), 0)[1], 0)
    wait_in(NC - 1)

    def last_half(n, _):
        h = 1 - n
        half_in(NC - 1, h)
        units(h)

        @pl.when(n == 0)
        def _():
            stage_part(0)

        return 0

    lax.fori_loop(0, 2, last_half, 0)

    A, B, O = LAGS

    def step_out(i, _):
        @pl.when((i >= 1) & (i < NC2))
        def _():
            stage_part(i)

        @pl.when((i >= A) & (i < NC2 + A))
        def _():
            stage_result(i - A)

        @pl.when((i >= B) & (i < NC2 + B))
        def _():
            stage_back(i - B)

        @pl.when(i == NC2 - 2)
        def _():
            mixer_wait()

        @pl.when((i >= NC2 - 2) & (i < NC2 + 2))
        def _():
            mixer_block(i - (NC2 - 2))

        @pl.when(i >= O)
        def _():
            stage_out(i - O)

        return 0

    lax.fori_loop(0, NC2 + O, step_out, 0)

    drain(zsend.at[:, pl.ds(0, NZ - 1)], zrecv.at[:, pl.ds(0, NZ - 1)], ssem.at[0])
    drain(wg.at[1], wg.at[1], ssem.at[1])
    drain(wu.at[1], wu.at[1], ssem.at[2])
    drain(wd.at[:, pl.ds(FL, FL)], wd.at[:, pl.ds(FL, FL)], ssem.at[3])
    m_mate.wait_send()
    m_relay.wait_send()
    m_weight.wait_send()
    m_passed.wait_send()

    @pl.when((t == 3) & (ep < E - 1))
    def _():
        drain(msend.at[:, pl.ds(0, WMAX)], msend.at[:, pl.ds(0, WMAX)], ssem.at[5])

    drain(ysend.at[:, pl.ds(0, NJ - 1)], ysend.at[:, pl.ds(0, NJ - 1)], ssem.at[6])
    drain(xs.at[0], xs.at[1], ssem.at[7])
    drain(psend, precv, ssem.at[8])
    drain(rsend.at[:, pl.ds(0, NJ - 1)], rsend.at[:, pl.ds(0, NJ - 1)], ssem.at[9])
    drain(rperm.at[:, pl.ds(0, NZ - 1)], rperm.at[:, pl.ds(0, NZ - 1)], ssem.at[10])
    lax.fori_loop(0, 4, lambda b, _: (mixed_copy(b).wait(), 0)[1], 0)
    lax.fori_loop(0, NC2, lambda c, _: (out_copy(c).wait(), 0)[1], 0)


def handover_kernel(parts, mixed, out, mixed_to, out_to, mixed_at, out_at, isem, osem):
    def pieces(source, target, sems):
        rows = source.shape[0] // parts
        return [
            pltpu.make_async_copy(
                source.at[pl.ds(p * rows, rows)], target.at[pl.ds(p * rows, rows)], sems.at[p]
            )
            for p in range(parts)
        ]

    taken = pieces(mixed, mixed_at, isem.at[0]) + pieces(out, out_at, isem.at[1])
    given = pieces(mixed_at, mixed_to, osem.at[0]) + pieces(out_at, out_to, osem.at[1])
    for copy in taken:
        copy.start()
    for copy, after in zip(taken, given):
        copy.wait()
        after.start()
    for copy in given:
        copy.wait()


def shards(
    mixer_in, mixer_gain, group_weight, group_scale, expert_in, expert_gain,
    routes, route_weight, gate_weight, up_weight, down_weight,
):
    E = lax.axis_size("ep")
    NJ = 8 if E == 64 else 2
    NZ = E // NJ
    TOK, D = expert_in.shape
    CAP = max(2, 3 * TOK * TOP // (2 * E))
    S = E * CAP
    FL = gate_weight.shape[2]
    NC = 16 if D >= 4096 else 4
    C = D // NC
    C2 = D // (CH2 if D >= 4096 else 4)
    NC2 = D // C2
    GW = D // 4
    BJ, BZ = NJ * CAP, NZ * CAP
    hbm = pl.BlockSpec(memory_space=pl.ANY)
    dma = pltpu.SemaphoreType.DMA
    buf = lambda *shape: pltpu.VMEM(shape, bf16)
    mixed, out = pl.pallas_call(
        functools.partial(layer_kernel, (NZ, NJ, TOK, D, C, C2, CAP, FL)),
        out_shape=(
            jax.ShapeDtypeStruct((4 * TOK, GW), bf16),
            jax.ShapeDtypeStruct((TOK, D), bf16),
        ),
        in_specs=[hbm] * 11,
        out_specs=(hbm, hbm),
        scratch_shapes=[
            buf(NC, TOK, C),
            buf(NC, NZ, BJ, C), buf(NC, NZ, BJ, C), buf(NC, NJ, BZ, C),
            buf(2, NC, NJ, BZ, C),
            buf(2, D, FL), buf(2, D, FL), buf(NC2, 2 * FL, C2),
            pltpu.VMEM((2, 4, S, FL), f32), buf(2, S, 2 * FL),
            buf(NC2, S, C2), buf(NC2, S, C2),
            buf(NC2, NJ, BZ, C2), buf(NC2, NJ, BZ, C2),
            buf(NC2, NZ, BJ, C2), buf(NC2, NZ, BJ, C2),
            buf(S, TOK), buf(TOK, S), buf(TOK, S),
            pltpu.VMEM((1, D), f32), pltpu.VMEM((1, D), f32),
            pltpu.VMEM((2, 4 * TOK), jnp.int32), pltpu.VMEM((2, 4 * TOK), f32),
            pltpu.VMEM((1, GW), f32),
            buf(TOK, D), buf(TOK, D), buf(S, S), buf(4, TOK, GW), buf(TOK, GW), buf(HALO + 4 * TOK, GW), buf(GW, GW), buf(4 * TOK, GW),
            buf(NC2, TOK, C2),
            dma((11,)), dma((2,)), dma((14,)),
            dma((NC,)), dma((NC,)), dma((NC,)), dma((NC,)), dma((NC,)), dma((NC2,)),
            dma((NC2,)), dma((NC2,)), dma((NC2,)), dma((5,)),
        ],
        compiler_params=pltpu.CompilerParams(
            collective_id=0, has_side_effects=True, vmem_limit_bytes=67043328
        ),
        name="layer",
    )(
        expert_gain[None], mixer_gain[None], routes.T, route_weight.T,
        group_scale, expert_in, mixer_in, group_weight, gate_weight, up_weight, down_weight,
    )
    PARTS = 4
    return pl.pallas_call(
        functools.partial(handover_kernel, PARTS),
        out_shape=(
            jax.ShapeDtypeStruct((4 * TOK, GW), bf16),
            jax.ShapeDtypeStruct((TOK, D), bf16),
        ),
        in_specs=[hbm] * 2,
        out_specs=(hbm, hbm),
        scratch_shapes=[
            buf(4 * TOK, GW), buf(TOK, D), dma((2, PARTS)), dma((2, PARTS)),
        ],
        name="handover",
    )(mixed, out)


def solution(mesh):
    in_specs = (
        P(("ep", "tp"), None),
        P(),
        P("tp", None, None),
        P("tp", None),
        P(("ep", "tp"), None),
        P(),
        P("ep", None),
        P("ep", None),
        P("ep", None, "tp"),
        P("ep", None, "tp"),
        P("ep", "tp", None),
    )
    out_specs = (P("ep", "tp"), P(("ep", "tp"), None))
    return jax.shard_map(shards, mesh=mesh, in_specs=in_specs, out_specs=out_specs, check_vma=False)
```
